32 devices in a mesh: grp: 2 (over y), ep: 4 (over z), tp: 4 (over x, core).
Axes of the slice: x: 2, y: 2, z: 4, core: 2. Of those that a mesh axis runs over, the one named last changes fastest.
Arguments:
- mix_input: bfloat16 [2048, 2048], P(('grp', 'ep'), 'tp'), parts along dimension 0, may hold values from -6 to 6
- group_weight: bfloat16 [16, 128, 128], replicated, may hold values from -0.5 to 0.5
- pool_gain: float32 [2048], replicated, may hold values from 0.1 to 1.9
- branch_weight: bfloat16 [2048, 2048], P('tp'), may hold values from -0.125 to 0.125
- exp_input: bfloat16 [1024, 2048], P(('grp', 'ep')), parts along dimension 0, may hold values from -6 to 6
- norm_gain: float32 [2048], replicated, may hold values from 0.1 to 1.9
- routes: int32 [1024, 2], P(('grp', 'ep')), parts along dimension 0, may hold values from 0 to 3, all different within a row; in each aligned block of 128 rows (0 to 127, 128 to 255, ...) at most 96 rows name the same one
- route_weights: float32 [1024, 2], P(('grp', 'ep')), parts along dimension 0, may hold values from 0.25 to 1
- gate_weight: bfloat16 [4, 2048, 3584], P('ep', None, 'tp'), may hold values from -0.125 to 0.125
- up_weight: bfloat16 [4, 2048, 3584], P('ep', None, 'tp'), may hold values from -0.125 to 0.125
- down_weight: bfloat16 [4, 3584, 2048], P('ep', 'tp'), may hold values from -0.09375 to 0.09375
Outputs:
- mix_out: bfloat16 [2048, 2048], P(('grp', 'ep'), 'tp'), parts along dimension 0
- exp_out: bfloat16 [1024, 2048], P(('grp', 'ep'), 'tp'), parts along dimension 0
The draws below stay inside these ranges and needn't reach their ends.
There are 2 independent parts, one for each index of `grp`. The reference program is written for one: setup_inputs(seed, part) draws one part's arguments, and reference() takes and returns one part's arrays. A program takes and returns all parts, laid end to end along the dimension named above; an argument that names none is the same for every part. Nothing has to cross between parts.
Inputs may be any that keep to these rules, and one draw needn't show every extreme that they name: `routes`: the 2 experts of a token differ. Among the 128 tokens of one index of ep no expert is named by more than 96 of them, a bound that some block reaches.
All inputs are finite; a program needn't handle non-finite values.
Results may differ from the reference program's by a relative error of at most 0.018.
Values may be sent and summed in bfloat16 or wider, within the bound.
A program may use at most 64 MiB of HBM per device.

```python
import math
import jax
import jax.numpy as jnp
import numpy as np
from jax import lax

WIDTH = 2048
GROUPS = 16
GROUP_WIDTH = 128
HIDDEN_SIZE = 3584
TOP_K = 2
TOK_EXP = 128
POOL_WIDTH = 2048
EXPERTS = 4
MIX_TOKENS = 1024
EXP_TOKENS = 512
EXP_ROWS = 384
CAP_SLOTS = 96
N_TP = 4


def steps_of(rng, dims, shards, smallest, largest):
    loudness, own = 1.0, jax.random.fold_in(rng, 6)
    for position, shards_of in shards:
        steps = jnp.exp(jax.random.uniform(jax.random.fold_in(own, position), (shards_of,), jnp.float32, smallest / len(shards), largest / len(shards)))
        loudness = loudness * jnp.repeat(steps, dims[position] // shards_of).reshape([-1 if axis == position else 1 for axis in range(len(dims))])
    return loudness


def assign_block(rng, own, number, rows, count, top, bound, slope):
    order = jax.random.permutation(rng, count)
    heavy_load, ordinary = load_shares(count, rows * top, bound, slope, True), load_shares(count, rows * top, bound, slope, False)
    places = jnp.arange(count)

    def named(sizes, offset_by):
        used = int((sizes > 0).sum())
        fixed = max(1, used // 4)
        passed = fixed + (places - fixed + offset_by * (used - fixed)) % max(1, count - fixed)
        return jnp.zeros((count,), jnp.int32).at[order[jnp.where(places < fixed, places, passed)]].set(jnp.asarray(sizes, jnp.int32))

    sizes = jnp.where(number % 4 == 0, named(heavy_load, number // 4), named(ordinary, number - number // 4 - 1))
    mixed = jax.random.permutation(jax.random.fold_in(own, 3), count)
    giver, sink = mixed[0:count // 2 * 2:2], mixed[1:count // 2 * 2:2]
    room = jnp.minimum(sizes[giver] - 1, bound - sizes[sink]) // 2
    room = jnp.where((giver == order[0]) | (sink == order[0]) | (sizes[sink] == 0), 0, jnp.maximum(room, 0))
    passed = jax.random.randint(jax.random.fold_in(own, 4), (count // 2,), 0, 1 << 20) % (room + 1)
    sizes = sizes.at[giver].add(-passed).at[sink].add(passed)
    labels = jnp.searchsorted(jnp.cumsum(sizes), jnp.arange(rows * top), side="right").astype(jnp.int32)
    grid = labels.reshape(top, rows).T
    grid = grid[jax.random.permutation(jax.random.fold_in(own, 1), rows)]
    offset_by = jax.random.randint(jax.random.fold_in(own, 2), (rows, 1), 0, top)
    return jnp.take_along_axis(grid, (jnp.arange(top)[None, :] + offset_by) % top, axis=1)


def load_shares(count, total, limit, skew, full):
    weights = [(1 << 20) // math.isqrt(standing ** skew) + 1 for standing in range(1, count + 1)]
    largest = limit if full else min(limit, max(-(-total // count), total * weights[0] // sum(weights)))
    least = 1 if total - largest >= count - 1 else 0
    given, spare = [largest] + [least] * (count - 1), total - largest - least * (count - 1)
    while spare > 0:
        free = [i for i in range(1, count) if given[i] < largest] or [i for i in range(1, count) if given[i] < limit]
        mass, budget = sum([weights[i] for i in free]), spare
        for i in free:
            more = min(limit - given[i], max(1, budget * weights[i] // mass), spare)
            given[i] = given[i] + more
            spare = spare - more
    return np.array(given)


def gaussian(rng, shape, spread, bound, split=(), kind=jnp.bfloat16):
    drawn = spread * jax.random.normal(rng, shape, jnp.float32)
    if split:
        drawn = drawn * steps_of(rng, shape, split, -0.22, 0.18)
    return jnp.clip(drawn, -bound, bound).astype(kind)


def setup_inputs(seed: int = 0, part: int = 0) -> dict:
    key_list = jax.random.split(jax.random.key(seed), 12)
    own_keys = jax.random.split(jax.random.fold_in(key_list[11], part), 12)
    mix_input = gaussian(own_keys[0], (MIX_TOKENS, POOL_WIDTH), 1.0, 6.0, ((0, 4), (1, 4)))
    group_weight = gaussian(key_list[1], (GROUPS, GROUP_WIDTH, GROUP_WIDTH), GROUP_WIDTH ** -0.5, 0.5)
    pool_gain = jnp.clip(1.0 + 0.18 * jax.random.normal(key_list[2], (POOL_WIDTH,), jnp.float32), 0.1, 1.9)
    branch_weight = gaussian(key_list[3], (POOL_WIDTH, WIDTH), POOL_WIDTH ** -0.5, 0.125, ((0, 4),))
    exp_input = gaussian(own_keys[4], (EXP_TOKENS, WIDTH), 1.0, 6.0, ((0, 4),))
    norm_gain = jnp.clip(1.0 + 0.18 * jax.random.normal(key_list[5], (WIDTH,), jnp.float32), 0.1, 1.9)
    routes_keys = jax.random.split(jax.random.fold_in(own_keys[6], 1), EXP_TOKENS // TOK_EXP)
    routes_turns = jax.random.permutation(jax.random.fold_in(own_keys[6], 3), EXP_TOKENS // TOK_EXP)
    routes = jax.vmap(lambda own, number: assign_block(jax.random.fold_in(own_keys[6], 2), own, number, TOK_EXP, EXPERTS, TOP_K, CAP_SLOTS, 1))(routes_keys, routes_turns).reshape((EXP_TOKENS, TOP_K))
    route_weights = jnp.clip(0.25 + 0.75 * jax.random.uniform(own_keys[7], (EXP_TOKENS, TOP_K), jnp.float32) ** steps_of(own_keys[7], (EXP_TOKENS, TOP_K), ((0, 4),), -0.2, 0.2), 0.25, 1.0)
    gate_weight = gaussian(key_list[8], (EXPERTS, WIDTH, HIDDEN_SIZE), WIDTH ** -0.5, 0.125, ((0, 4), (2, 4)))
    up_weight = gaussian(key_list[9], (EXPERTS, WIDTH, HIDDEN_SIZE), WIDTH ** -0.5, 0.125, ((0, 4), (2, 4)))
    down_weight = gaussian(key_list[10], (EXPERTS, HIDDEN_SIZE, WIDTH), HIDDEN_SIZE ** -0.5, 0.09375, ((0, 4), (1, 4)))
    return dict(mix_input=mix_input, group_weight=group_weight, pool_gain=pool_gain, branch_weight=branch_weight, exp_input=exp_input, norm_gain=norm_gain, routes=routes, route_weights=route_weights, gate_weight=gate_weight, up_weight=up_weight, down_weight=down_weight)


windows = (2, 4, 8, 16)
epsilon = 1e-06

def trailing_sums(extended, rows):
    span_two = extended[1:] + extended[:-1]
    span_four = span_two[2:] + span_two[:-2]
    span_eight = span_four[4:] + span_four[:-4]
    span_sixteen = span_eight[8:] + span_eight[:-8]
    return [span_two[-rows:], span_four[-rows:], span_eight[-rows:], span_sixteen[-rows:]]

def pooled_deviation(extended, positions, group_ids, group_width, rows):
    sums = trailing_sums(extended, rows)
    current = extended[-rows:]
    window_id = jnp.repeat(group_ids % 4, group_width)
    result = jnp.zeros_like(current)
    for window_level, window_len in enumerate(windows):
        counted = jnp.minimum(positions + 1, window_len).astype(jnp.float32)[:, None]
        result = jnp.where(window_id[None, :] == window_level, sums[window_level] / counted - current, result)
    return result

def blockwise_product(left, right, blocks):
    inner = left.shape[1] // blocks
    left_pieces = left.reshape(left.shape[0], blocks, inner).transpose(1, 0, 2)
    right_pieces = right.reshape(blocks, inner, right.shape[1])

    def add_block(running, operands):
        piece, weight = operands
        rounded = lax.optimization_barrier(jnp.dot(piece, weight, preferred_element_type=jnp.float32).astype(jnp.bfloat16))
        return (running + rounded.astype(jnp.float32), None)
    start_sum = jnp.zeros((left.shape[0], right.shape[1]), jnp.float32)
    running, _ = lax.scan(add_block, start_sum, (left_pieces, right_pieces))
    return running.astype(jnp.bfloat16)

def reference(mix_input, group_weight, pool_gain, branch_weight, exp_input, norm_gain, routes, route_weights, gate_weight, up_weight, down_weight):
    rows = mix_input.shape[0]
    extended = jnp.concatenate([jnp.zeros((15, POOL_WIDTH), jnp.float32), mix_input.astype(jnp.float32)], axis=0)
    positions = jnp.arange(rows, dtype=jnp.int32)
    group_ids = jnp.arange(GROUPS, dtype=jnp.int32)
    deviation = pooled_deviation(extended, positions, group_ids, GROUP_WIDTH, rows).astype(jnp.bfloat16)
    grouped = jnp.einsum('rgc,gcd->rgd', deviation.reshape(rows, GROUPS, GROUP_WIDTH).astype(jnp.float32), group_weight.astype(jnp.float32)).reshape(rows, POOL_WIDTH)
    pooled = (grouped * pool_gain).astype(jnp.bfloat16)
    mix_out = blockwise_product(pooled, branch_weight, N_TP)
    tokens = exp_input.shape[0]
    floated = exp_input.astype(jnp.float32)
    normed = (floated * lax.rsqrt(lax.optimization_barrier(jnp.mean(floated * floated, axis=1, keepdims=True)) + epsilon) * norm_gain).astype(jnp.bfloat16)
    flat_expert = routes.reshape(-1).astype(jnp.int32)
    assignments = flat_expert.shape[0]
    onehot = (flat_expert[:, None] == jnp.arange(EXPERTS, dtype=jnp.int32)[None, :]).astype(jnp.int32)
    slot_rank = lax.optimization_barrier(jnp.sum((jnp.cumsum(onehot, axis=0) - onehot) * onehot, axis=1)).astype(jnp.int32)
    token_of = (jnp.arange(assignments, dtype=jnp.int32) // TOP_K).astype(jnp.int32)
    slot_table = jnp.full((EXPERTS, EXP_ROWS), tokens, jnp.int32).at[flat_expert, slot_rank].set(token_of)
    padded = jnp.concatenate([normed, jnp.zeros((1, WIDTH), jnp.bfloat16)], axis=0)

    def one_expert(operands):
        row_index, w_gate, w_up, w_down = operands
        chosen = padded[row_index]
        gate_pre = jnp.dot(chosen, w_gate, preferred_element_type=jnp.float32)
        up_pre = jnp.dot(chosen, w_up, preferred_element_type=jnp.float32)
        hidden = (jax.nn.silu(gate_pre) * up_pre).astype(jnp.bfloat16)
        return blockwise_product(hidden, w_down, N_TP)
    outputs = lax.map(one_expert, (slot_table, gate_weight, up_weight, down_weight))
    picked = outputs[flat_expert, slot_rank].astype(jnp.float32).reshape(tokens, TOP_K, WIDTH)
    exp_out = lax.optimization_barrier(jnp.sum(picked * route_weights[:, :, None], axis=1)).astype(jnp.bfloat16)
    return (mix_out, exp_out)
```

```python
import functools

import jax
import jax.numpy as jnp
from jax import lax
from jax.experimental import pallas as pl
from jax.experimental.pallas import tpu as pltpu
from jax.sharding import PartitionSpec as P

windows = (2, 4, 8, 16)
epsilon = 1e-06


def shifted(block, axis, distance):
    devices = range(lax.axis_size(axis))
    route = [(i - distance, i) for i in devices if i - distance in devices]
    return lax.ppermute(block, axis, route)


def trailing_sums(extended, rows):
    span_two = extended[1:] + extended[:-1]
    span_four = span_two[2:] + span_two[:-2]
    span_eight = span_four[4:] + span_four[:-4]
    span_sixteen = span_eight[8:] + span_eight[:-8]
    return [span_two[-rows:], span_four[-rows:], span_eight[-rows:], span_sixteen]


def pooled_deviation(extended, positions, group_ids, group_width, rows):
    sums = trailing_sums(extended, rows)
    current = extended[-rows:]
    window_id = jnp.repeat(group_ids % 4, group_width)
    result = jnp.zeros_like(current)
    for window_level, window_len in enumerate(windows):
        counted = jnp.minimum(positions + 1, window_len).astype(jnp.float32)[:, None]
        result = jnp.where(
            window_id[None, :] == window_level, sums[window_level] / counted - current, result
        )
    return result


def on_device(
    mix_input,
    group_weight,
    pool_gain,
    branch_weight,
    exp_input,
    norm_gain,
    routes,
    route_weights,
    gate_weight,
    up_weight,
    down_weight,
):
    tp_rank = lax.axis_index("tp")
    ep_rank = lax.axis_index("ep")
    rows_mix, channels = mix_input.shape
    group_width = group_weight.shape[1]
    group_count = channels // group_width
    first_group = tp_rank * group_count
    last_rows = mix_input[rows_mix - 15 :]
    before = shifted(last_rows, "ep", 1)
    extended = jnp.concatenate([before, mix_input], axis=0).astype(jnp.float32)
    positions = ep_rank * rows_mix + jnp.arange(rows_mix, dtype=jnp.int32)
    group_ids = first_group + jnp.arange(group_count, dtype=jnp.int32)
    deviation = pooled_deviation(extended, positions, group_ids, group_width, rows_mix).astype(
        jnp.bfloat16
    )
    own_groups = lax.dynamic_slice_in_dim(group_weight, first_group, group_count, 0)
    grouped = jnp.einsum(
        "rgc,gcd->rgd",
        deviation.reshape(rows_mix, group_count, group_width),
        own_groups,
        preferred_element_type=jnp.float32,
    ).reshape(rows_mix, channels)
    own_gain = lax.dynamic_slice_in_dim(pool_gain, first_group * group_width, channels, 0)
    pooled = (grouped * own_gain).astype(jnp.bfloat16)
    tok_rows, width = exp_input.shape
    columns = width // lax.axis_size("tp")
    experts_all = lax.axis_size("ep")
    capacity = 3 * tok_rows // experts_all
    floated = exp_input.astype(jnp.float32)
    normed = (
        floated
        * lax.rsqrt(jnp.mean(floated * floated, axis=1, keepdims=True) + epsilon)
        * norm_gain
    ).astype(jnp.bfloat16)
    flat_expert = routes.reshape(-1)
    assignments = flat_expert.shape[0]
    onehot = (flat_expert[:, None] == jnp.arange(experts_all, dtype=jnp.int32)[None, :]).astype(
        jnp.int32
    )
    slot_rank = jnp.sum((jnp.cumsum(onehot, axis=0) - onehot) * onehot, axis=1)
    slot_index = flat_expert * capacity + slot_rank
    token_of = jnp.arange(assignments, dtype=jnp.int32) // routes.shape[1]
    slot_token = (
        jnp.full((experts_all * capacity,), tok_rows, jnp.int32).at[slot_index].set(token_of)
    )
    padded = jnp.concatenate([normed, jnp.zeros((1, width), jnp.bfloat16)], axis=0)
    w_gate = gate_weight[0]
    w_up = up_weight[0]
    w_down = down_weight[0]
    arrived_rows = experts_all * capacity
    own_columns = lax.dynamic_slice_in_dim(padded, tp_rank * columns, columns, 1)
    outgoing = own_columns[slot_token].reshape(experts_all, capacity, columns)
    arrived = lax.all_to_all(outgoing, "ep", split_axis=0, concat_axis=0, tiled=True).reshape(
        arrived_rows, columns
    )
    section = lax.all_gather(arrived, "tp", axis=1, tiled=True)
    gate_pre = jnp.dot(section, w_gate, preferred_element_type=jnp.float32)
    up_pre = jnp.dot(section, w_up, preferred_element_type=jnp.float32)
    hidden = (jax.nn.silu(gate_pre) * up_pre).astype(jnp.bfloat16)
    weight_cols = branch_weight
    mix_sum = lax.psum_scatter(
        lax.dot_general(
            weight_cols, pooled, (((0,), (1,)), ((), ())), preferred_element_type=jnp.float32
        ).astype(jnp.bfloat16),
        "tp",
        scatter_dimension=0,
        tiled=True,
    )
    weight_cols = w_down
    exp_sum = lax.psum_scatter(
        lax.dot_general(
            weight_cols, hidden, (((0,), (1,)), ((), ())), preferred_element_type=jnp.float32
        ).astype(jnp.bfloat16),
        "tp",
        scatter_dimension=0,
        tiled=True,
    )
    mix_out = mix_sum.T
    results = exp_sum.reshape(columns, experts_all, capacity)
    returned = lax.all_to_all(results, "ep", split_axis=1, concat_axis=1, tiled=True).reshape(
        columns, experts_all * capacity
    )
    picked = returned[:, slot_index].astype(jnp.float32)
    weighted = picked * route_weights.reshape(-1)[None, :]
    combined = jnp.sum(weighted.reshape(columns, tok_rows, routes.shape[1]), axis=2)
    exp_out = combined.T.astype(jnp.bfloat16)
    return (mix_out, exp_out)


lanes = 128
MESH = pl.DeviceIdType.MESH
f32 = jnp.float32
bf16 = jnp.bfloat16


def fused_kernel(
    x_hbm,
    norm_hbm,
    routes_hbm,
    weights_hbm,
    mix_hbm,
    gain_hbm,
    groups_hbm,
    branch_hbm,
    gate_hbm,
    up_hbm,
    down_hbm,
    mix_out,
    exp_out,
    x_ref,
    norm_ref,
    routes_ref,
    weights_ref,
    mix_ref,
    gain_ref,
    wgu,
    wd,
    wb,
    gw,
    xn,
    sb,
    xg,
    gu,
    hid,
    halo,
    pooled,
    keep_m,
    ps_m,
    pr_m,
    xs_m,
    xr_m,
    keep,
    ps,
    pr,
    xs,
    xr,
    zs,
    zr,
    w_sem,
    i_sem,
    d_send,
    d_recv,
    f_send,
    f_recv,
    p_send,
    p_recv,
    r_send,
    r_recv,
    z_send,
    z_recv,
    m_send,
    m_recv,
    h_sem,
):
    z = lax.axis_index("ep")
    t = lax.axis_index("tp")
    near = t + 1 - 2 * (t % 2)
    across = (t + 2) % 4
    diagonal = (near + 2) % 4
    inner = ((z + 1) // 2) % 2
    peers = [z, z + 1 - 2 * (z % 2), 3 - z, (z + 2) % 4]
    landing = 3 - inner
    homes = [0, 1, 3 - inner, 2 + inner]
    home_of = [
        z,
        peers[1],
        inner * peers[2] + (1 - inner) * peers[3],
        inner * peers[3] + (1 - inner) * peers[2],
    ]
    tokens, width = x_ref.shape
    quarter = width // 4
    cap = xg.shape[2]
    piece = cap // 2
    hid_tiles = gate_hbm.shape[2] // lanes
    rows_mix, channels = mix_ref.shape
    half_mix = rows_mix // 2
    group_count = channels // lanes

    barrier = pltpu.get_barrier_semaphore()
    for k in (1, 2, 3):
        pl.semaphore_signal(barrier, inc=1, device_id={"ep": peers[k]}, device_id_type=MESH)
    for k in (near, across):
        pl.semaphore_signal(barrier, inc=1, device_id={"tp": k}, device_id_type=MESH)

    pairs = (
        (x_hbm, x_ref),
        (norm_hbm, norm_ref),
        (routes_hbm, routes_ref),
        (weights_hbm, weights_ref),
        (mix_hbm, mix_ref),
        (gain_hbm, gain_ref),
    )
    load_i = [pltpu.make_async_copy(src, dst, i_sem.at[i]) for i, (src, dst) in enumerate(pairs)]
    loads = []
    for i in range(2 * hid_tiles):
        src = gate_hbm if i < hid_tiles else up_hbm
        at = (i % hid_tiles) * lanes
        loads.append(
            pltpu.make_async_copy(
                src.at[0, :, pl.ds(at, lanes)],
                wgu.at[i // 2, :, pl.ds((i % 2) * lanes, lanes)],
                w_sem.at[i],
            )
        )
    n0 = 2 * hid_tiles
    load_b = [
        pltpu.make_async_copy(branch_hbm.at[:, pl.ds(k * quarter, quarter)], wb.at[k], w_sem.at[n0 + k])
        for k in range(4)
    ]
    load_d = [
        pltpu.make_async_copy(down_hbm.at[0, :, pl.ds(k * quarter, quarter)], wd.at[k], w_sem.at[n0 + 4 + k])
        for k in range(4)
    ]
    load_g = pltpu.make_async_copy(groups_hbm.at[pl.ds(t * group_count, group_count)], gw, w_sem.at[n0 + 8])
    for c in load_i:
        c.start()

    def remote(src, dst, send, recv, who):
        return pltpu.make_async_remote_copy(
            src_ref=src, dst_ref=dst, send_sem=send, recv_sem=recv, device_id=who, device_id_type=MESH
        )

    for c in load_i[:4]:
        c.wait()
    for c in [load_g] + load_b + loads + load_d:
        c.start()
    floated = x_ref[...].astype(f32)
    scale = lax.rsqrt(jnp.mean(floated * floated, axis=1, keepdims=True) + epsilon)
    xn_val = (floated * scale * norm_ref[...]).astype(bf16)
    for k in range(4):
        xn[k] = xn_val[:, k * quarter : (k + 1) * quarter]
    lane = lax.broadcasted_iota(jnp.int32, (tokens, lanes), 1)
    square = (tokens, tokens)
    diagonal_mask = lax.broadcasted_iota(jnp.int32, square, 0) == lax.broadcasted_iota(jnp.int32, square, 1)

    def column(row):
        spread = jnp.broadcast_to(row, square)
        return jnp.sum(jnp.where(diagonal_mask, spread, jnp.zeros_like(spread)), axis=1, keepdims=True)

    r0 = column(routes_ref[0:1, :].astype(f32)).astype(jnp.int32)
    r1 = column(routes_ref[1:2, :].astype(f32)).astype(jnp.int32)
    w0 = column(weights_ref[0:1, :])
    w1 = column(weights_ref[1:2, :])
    member = ((r0 == lane) | (r1 == lane)).astype(f32)
    above = (
        lax.broadcasted_iota(jnp.int32, (tokens, tokens), 0)
        > lax.broadcasted_iota(jnp.int32, (tokens, tokens), 1)
    ).astype(f32)
    rank = jnp.dot(above.astype(bf16), member.astype(bf16), preferred_element_type=f32)
    slot_lane = lax.broadcasted_iota(jnp.int32, (tokens, cap), 1)
    places = []
    shares = []
    for k in range(4):
        own = jnp.sum(jnp.where(lane == peers[k], rank, 0.0), axis=1, keepdims=True).astype(jnp.int32)
        named = (r0 == peers[k]) | (r1 == peers[k])
        slot = jnp.where(named, own, cap)
        places.append((slot_lane == slot).astype(f32).astype(bf16))
        shares.append(
            jnp.where(r0 == peers[k], w0, 0.0)
            + jnp.where(r1 == peers[k], w1, 0.0)
        )

    def gathered(k, block):
        return lax.dot_general(
            places[k], block, (((0,), (0,)), ((), ())), preferred_element_type=f32
        ).astype(bf16)

    own_cols = xn[t]
    sb[0] = gathered(1, own_cols)
    for k in (2, 3):
        sb[k] = gathered(k, own_cols)
    sb[1] = gathered(1, xn[across])
    for c in load_i[4:]:
        c.wait()
    pl.semaphore_wait(barrier, 5)

    def d_z(j, p):
        rows = pl.ds(p * piece, piece)
        q = across if j == 1 else t
        slot = 1 if j < 2 else landing
        at = j if j < 2 else landing
        return remote(
            sb.at[j, rows],
            xg.at[q, slot, rows],
            d_send.at[j, p],
            d_recv.at[at, p],
            {"ep": peers[max(j, 1)]},
        )

    sent = []

    def launch(c):
        c.start()
        sent.append(c)

    halo_copy = remote(
        mix_ref.at[pl.ds(rows_mix - 16, 16), :], halo, h_sem.at[0], h_sem.at[1], {"ep": (z + 1) % 4}
    )

    @pl.when(z < 3)
    def _():
        halo_copy.start()

    for j in range(4):
        for p in range(2):
            launch(d_z(j, p))
    for q in range(4):
        xg[q, 0] = gathered(0, xn[q])

    def arrival(at, q, slot, p):
        rows = pl.ds(p * piece, piece)
        return remote(
            sb.at[0, rows], xg.at[q, slot, rows], d_send.at[0, p], d_recv.at[at, p], {"ep": peers[1]}
        )

    def forward(i, q, slot, p):
        rows = pl.ds(p * piece, piece)
        block = xg.at[q, slot, rows]
        return remote(
            block, block, f_send.at[i, slot, p], f_recv.at[i, slot, p], {"tp": across if i == 0 else near}
        )

    def from_z(k):
        if k == 1:
            for p in range(2):
                arrival(0, t, 1, p).wait_recv()
                launch(forward(1, t, 1, p))
            for p in range(2):
                arrival(1, across, 1, p).wait_recv()
                launch(forward(2, across, 1, p))
            return
        for p in range(2):
            arrival(k, t, k, p).wait_recv()
            launch(forward(0, t, k, p))
            launch(forward(1, t, k, p))

    def from_x(k):
        for p in range(2):
            forward(0, across, k, p).wait_recv()
            launch(forward(2, across, k, p))

    def from_near(k):
        for p in range(2):
            forward(1, near, k, p).wait_recv()
            forward(2, diagonal, k, p).wait_recv()

    def mix_half(h):
        rows = slice(h * half_mix, (h + 1) * half_mix)
        position = z * rows_mix + h * half_mix + lax.broadcasted_iota(jnp.int32, (half_mix, lanes), 0)
        for g in range(group_count):
            cols = slice(g * lanes, (g + 1) * lanes)
            current = mix_ref[rows, cols].astype(f32)
            if h == 0:
                past = halo[:, cols].astype(f32)
            else:
                past = mix_ref[h * half_mix - 16 : h * half_mix, cols].astype(f32)
            total = jnp.concatenate([past, current], axis=0)
            level = g % 4
            for step in range(level + 1):
                total = total + pltpu.roll(total, 1 << step, 0)
            counted = jnp.minimum(position + 1, windows[level]).astype(f32)
            deviation = (total[16:] / counted - current).astype(bf16)
            grouped = jnp.dot(deviation, gw[g], preferred_element_type=f32)
            gain = gain_ref[:, pl.ds(pl.multiple_of(t * channels + g * lanes, lanes), lanes)]
            pooled[rows, cols] = (grouped * gain).astype(bf16)
        for i, q in enumerate((diagonal, near)):
            ps_m[h, i] = jnp.dot(pooled[rows], wb[q], preferred_element_type=f32).astype(bf16)
            launch(m_p(h, i))
        for i, q in enumerate((across, t)):
            keep_m[h, i] = jnp.dot(pooled[rows], wb[q], preferred_element_type=f32)

    def m_p(h, i):
        return remote(ps_m.at[h, i], pr_m.at[h, i], m_send.at[h, i], m_recv.at[h, i], {"tp": near})

    def m_x(h):
        return remote(xs_m.at[h], xr_m.at[h], m_send.at[h, 2], m_recv.at[h, 2], {"tp": across})

    def send_mix(h):
        m_p(h, 0).wait_recv()
        xs_m[h] = (keep_m[h, 0] + pr_m[h, 0].astype(f32)).astype(bf16)
        launch(m_x(h))

    def finish_mix(h):
        m_p(h, 1).wait_recv()
        m_x(h).wait_recv()
        total = keep_m[h, 1] + pr_m[h, 1].astype(f32) + xr_m[h].astype(f32)
        mix_out[h * half_mix : (h + 1) * half_mix] = total.astype(bf16)

    def expand(k, first, last):
        for n in range(first, last):
            if k == 0:
                loads[2 * n].wait()
                loads[2 * n + 1].wait()
            total = None
            for q in range(4):
                part = jnp.dot(
                    xg[q, k], wgu[n, q * quarter : (q + 1) * quarter, :], preferred_element_type=f32
                )
                total = part if total is None else total + part
            gu[n] = total

    def activate(k):
        for i in range(hid_tiles):
            m = hid_tiles + i
            gate = gu[i // 2, :, (i % 2) * lanes : (i % 2 + 1) * lanes]
            up = gu[m // 2, :, (m % 2) * lanes : (m % 2 + 1) * lanes]
            hid[k, :, i * lanes : (i + 1) * lanes] = (gate / (1.0 + jnp.exp(-gate)) * up).astype(bf16)

    def r_p(i, k):
        return remote(ps.at[i, k], pr.at[i, k], p_send.at[i, k], p_recv.at[i, k], {"tp": near})

    def r_x(k, p):
        rows = pl.ds(p * piece, piece)
        return remote(xs.at[k, rows], xr.at[k, rows], r_send.at[k, p], r_recv.at[k, p], {"tp": across})

    def r_z(k, p):
        rows = pl.ds(p * piece, piece)
        return remote(
            zs.at[k, rows],
            zr.at[homes[k], rows],
            z_send.at[k, p],
            z_recv.at[homes[k], p],
            {"ep": home_of[k]},
        )

    def project(k):
        for i, q in enumerate((diagonal, across, near, t)):
            part = jnp.dot(hid[k], wd[q], preferred_element_type=f32)
            if i % 2 == 0:
                ps[i // 2, k] = part.astype(bf16)
                launch(r_p(i // 2, k))
            else:
                keep[i // 2, k] = part

    def send_x(k):
        r_p(0, k).wait_recv()
        for p in range(2):
            rows = slice(p * piece, (p + 1) * piece)
            xs[k, rows] = (keep[0, k, rows] + pr[0, k, rows].astype(f32)).astype(bf16)
            launch(r_x(k, p))

    def send_z(k):
        r_p(1, k).wait_recv()
        for p in range(2):
            rows = slice(p * piece, (p + 1) * piece)
            r_x(k, p).wait_recv()
            zs[k, rows] = (keep[1, k, rows] + pr[1, k, rows].astype(f32) + xr[k, rows].astype(f32)).astype(bf16)
            if k > 0:
                launch(r_z(k, p))

    def share(k):
        block = zs[0] if k == 0 else zr[k]
        return shares[k] * jnp.dot(places[k], block, preferred_element_type=f32)

    def returned(k):
        for p in range(2):
            rows = pl.ds(p * piece, piece)
            remote(
                zs.at[k, rows], zr.at[k, rows], z_send.at[k, p], z_recv.at[k, p], {"ep": peers[k]}
            ).wait_recv()

    half = hid_tiles // 2
    load_g.wait()
    for c in load_b:
        c.wait()
    mix_half(1)
    expand(0, 0, hid_tiles)
    send_mix(1)
    activate(0)

    @pl.when(z == 0)
    def _():
        halo[...] = jnp.zeros_like(halo)

    @pl.when(z > 0)
    def _():
        halo_copy.wait_recv()

    mix_half(0)
    for c in load_d:
        c.wait()
    project(0)
    from_z(2)
    send_x(0)
    from_z(1)
    from_near(1)
    expand(1, 0, hid_tiles)
    activate(1)
    project(1)
    from_x(2)
    from_z(3)
    send_x(1)
    from_near(2)
    expand(2, 0, hid_tiles)
    activate(2)
    project(2)
    from_x(3)
    send_x(2)
    send_z(1)
    send_z(0)
    from_near(3)
    expand(3, 0, hid_tiles)
    activate(3)
    project(3)
    send_z(2)
    send_x(3)
    send_mix(0)
    finish_mix(1)
    result = share(0)
    returned(1)
    result = result + share(1)
    send_z(3)
    finish_mix(0)
    for k in (2, 3):
        returned(k)
        result = result + share(k)
    exp_out[...] = result.astype(bf16)

    @pl.when(z < 3)
    def _():
        halo_copy.wait_send()

    for c in sent:
        c.wait_send()


def fused(
    mix_input,
    group_weight,
    pool_gain,
    branch_weight,
    exp_input,
    norm_gain,
    routes,
    route_weights,
    gate_weight,
    up_weight,
    down_weight,
):
    tokens, width = exp_input.shape
    rows_mix, channels = mix_input.shape
    hidden = gate_weight.shape[2]
    quarter = width // 4
    cap = 3 * tokens // 4
    hid_tiles = hidden // lanes
    half_mix = rows_mix // 2
    vmem = pl.BlockSpec(memory_space=pltpu.VMEM)
    anywhere = pl.BlockSpec(memory_space=pl.ANY)
    dma = pltpu.SemaphoreType.DMA
    return pl.pallas_call(
        fused_kernel,
        out_shape=(
            pltpu.VMEM((rows_mix, quarter), bf16),
            pltpu.VMEM((tokens, quarter), bf16),
        ),
        in_specs=[anywhere] * 11,
        out_specs=(vmem, vmem),
        scratch_shapes=[
            pltpu.VMEM((tokens, width), bf16),
            pltpu.VMEM((1, width), f32),
            pltpu.VMEM((2, tokens), jnp.int32),
            pltpu.VMEM((2, tokens), f32),
            pltpu.VMEM((rows_mix, channels), bf16),
            pltpu.VMEM((1, 4 * channels), f32),
            pltpu.VMEM((hid_tiles, width, 2 * lanes), bf16),
            pltpu.VMEM((4, hidden, quarter), bf16),
            pltpu.VMEM((4, channels, quarter), bf16),
            pltpu.VMEM((channels // lanes, lanes, lanes), bf16),
            pltpu.VMEM((4, tokens, quarter), bf16),
            pltpu.VMEM((4, cap, quarter), bf16),
            pltpu.VMEM((4, 4, cap, quarter), bf16),
            pltpu.VMEM((hid_tiles, cap, 2 * lanes), f32),
            pltpu.VMEM((4, cap, hidden), bf16),
            pltpu.VMEM((16, channels), bf16),
            pltpu.VMEM((rows_mix, channels), bf16),
            pltpu.VMEM((2, 2, half_mix, quarter), f32),
            pltpu.VMEM((2, 2, half_mix, quarter), bf16),
            pltpu.VMEM((2, 2, half_mix, quarter), bf16),
            pltpu.VMEM((2, half_mix, quarter), bf16),
            pltpu.VMEM((2, half_mix, quarter), bf16),
            pltpu.VMEM((2, 4, cap, quarter), f32),
            pltpu.VMEM((2, 4, cap, quarter), bf16),
            pltpu.VMEM((2, 4, cap, quarter), bf16),
            pltpu.VMEM((4, cap, quarter), bf16),
            pltpu.VMEM((4, cap, quarter), bf16),
            pltpu.VMEM((4, cap, quarter), bf16),
            pltpu.VMEM((4, cap, quarter), bf16),
            dma((2 * hid_tiles + 9,)),
            dma((6,)),
            dma((4, 2)),
            dma((4, 2)),
            dma((3, 4, 2)),
            dma((3, 4, 2)),
            dma((2, 4)),
            dma((2, 4)),
            dma((4, 2)),
            dma((4, 2)),
            dma((4, 2)),
            dma((4, 2)),
            dma((2, 3)),
            dma((2, 3)),
            dma((2,)),
        ],
        compiler_params=pltpu.CompilerParams(
            collective_id=0, has_side_effects=True, vmem_limit_bytes=56 << 20
        ),
    )(
        exp_input,
        norm_gain.reshape(1, -1),
        routes.T,
        route_weights.T,
        mix_input,
        pool_gain.reshape(1, -1),
        group_weight,
        branch_weight,
        gate_weight,
        up_weight,
        down_weight,
    )


def fits(mesh, args):
    mix, group, _, _, tok, _, routes, _, gate, _, _ = args
    ep, tp, grp = (mesh.shape[k] for k in ("ep", "tp", "grp"))
    if ep != 4 or tp != 4 or routes.shape[1] != 2 or gate.shape[0] != ep:
        return False
    rows, channels = mix.shape[0] // (grp * ep), mix.shape[1] // tp
    tokens, quarter = tok.shape[0] // (grp * ep), tok.shape[1] // tp
    return (
        group.shape[1] == lanes
        and channels % (4 * lanes) == 0
        and channels == quarter
        and rows % 32 == 0
        and tokens % 64 == 0
        and gate.shape[2] % (tp * lanes) == 0
        and gate.shape[1] * gate.shape[2] <= 1 << 23
        and rows <= 512
        and tokens <= 256
    )


def solution(mesh):
    def run(*args):
        body = fused if fits(mesh, args) else on_device
        return jax.shard_map(
            body,
            mesh=mesh,
            in_specs=(
                P(("grp", "ep"), "tp"),
                P(),
                P(),
                P("tp", None),
                P(("grp", "ep"), None),
                P(),
                P(("grp", "ep"), None),
                P(("grp", "ep"), None),
                P("ep", None, "tp"),
                P("ep", None, "tp"),
                P("ep", "tp", None),
            ),
            out_specs=(P(("grp", "ep"), "tp"), P(("grp", "ep"), "tp")),
            check_vma=False,
        )(*args)

    return run
```

```python
import functools

import jax
import jax.numpy as jnp
from jax import lax
from jax.experimental import pallas as pl
from jax.experimental.pallas import tpu as pltpu
from jax.sharding import PartitionSpec as P

windows = (2, 4, 8, 16)
epsilon = 1e-06


def shifted(block, axis, distance):
    devices = range(lax.axis_size(axis))
    route = [(i - distance, i) for i in devices if i - distance in devices]
    return lax.ppermute(block, axis, route)


def trailing_sums(extended, rows):
    span_two = extended[1:] + extended[:-1]
    span_four = span_two[2:] + span_two[:-2]
    span_eight = span_four[4:] + span_four[:-4]
    span_sixteen = span_eight[8:] + span_eight[:-8]
    return [span_two[-rows:], span_four[-rows:], span_eight[-rows:], span_sixteen]


def pooled_deviation(extended, positions, group_ids, group_width, rows):
    sums = trailing_sums(extended, rows)
    current = extended[-rows:]
    window_id = jnp.repeat(group_ids % 4, group_width)
    result = jnp.zeros_like(current)
    for window_level, window_len in enumerate(windows):
        counted = jnp.minimum(positions + 1, window_len).astype(jnp.float32)[:, None]
        result = jnp.where(
            window_id[None, :] == window_level, sums[window_level] / counted - current, result
        )
    return result


def on_device(
    mix_input,
    group_weight,
    pool_gain,
    branch_weight,
    exp_input,
    norm_gain,
    routes,
    route_weights,
    gate_weight,
    up_weight,
    down_weight,
):
    tp_rank = lax.axis_index("tp")
    ep_rank = lax.axis_index("ep")
    rows_mix, channels = mix_input.shape
    group_width = group_weight.shape[1]
    group_count = channels // group_width
    first_group = tp_rank * group_count
    last_rows = mix_input[rows_mix - 15 :]
    before = shifted(last_rows, "ep", 1)
    extended = jnp.concatenate([before, mix_input], axis=0).astype(jnp.float32)
    positions = ep_rank * rows_mix + jnp.arange(rows_mix, dtype=jnp.int32)
    group_ids = first_group + jnp.arange(group_count, dtype=jnp.int32)
    deviation = pooled_deviation(extended, positions, group_ids, group_width, rows_mix).astype(
        jnp.bfloat16
    )
    own_groups = lax.dynamic_slice_in_dim(group_weight, first_group, group_count, 0)
    grouped = jnp.einsum(
        "rgc,gcd->rgd",
        deviation.reshape(rows_mix, group_count, group_width),
        own_groups,
        preferred_element_type=jnp.float32,
    ).reshape(rows_mix, channels)
    own_gain = lax.dynamic_slice_in_dim(pool_gain, first_group * group_width, channels, 0)
    pooled = (grouped * own_gain).astype(jnp.bfloat16)
    tok_rows, width = exp_input.shape
    columns = width // lax.axis_size("tp")
    experts_all = lax.axis_size("ep")
    capacity = 3 * tok_rows // experts_all
    floated = exp_input.astype(jnp.float32)
    normed = (
        floated
        * lax.rsqrt(jnp.mean(floated * floated, axis=1, keepdims=True) + epsilon)
        * norm_gain
    ).astype(jnp.bfloat16)
    flat_expert = routes.reshape(-1)
    assignments = flat_expert.shape[0]
    onehot = (flat_expert[:, None] == jnp.arange(experts_all, dtype=jnp.int32)[None, :]).astype(
        jnp.int32
    )
    slot_rank = jnp.sum((jnp.cumsum(onehot, axis=0) - onehot) * onehot, axis=1)
    slot_index = flat_expert * capacity + slot_rank
    token_of = jnp.arange(assignments, dtype=jnp.int32) // routes.shape[1]
    slot_token = (
        jnp.full((experts_all * capacity,), tok_rows, jnp.int32).at[slot_index].set(token_of)
    )
    padded = jnp.concatenate([normed, jnp.zeros((1, width), jnp.bfloat16)], axis=0)
    w_gate = gate_weight[0]
    w_up = up_weight[0]
    w_down = down_weight[0]
    arrived_rows = experts_all * capacity
    own_columns = lax.dynamic_slice_in_dim(padded, tp_rank * columns, columns, 1)
    outgoing = own_columns[slot_token].reshape(experts_all, capacity, columns)
    arrived = lax.all_to_all(outgoing, "ep", split_axis=0, concat_axis=0, tiled=True).reshape(
        arrived_rows, columns
    )
    section = lax.all_gather(arrived, "tp", axis=1, tiled=True)
    gate_pre = jnp.dot(section, w_gate, preferred_element_type=jnp.float32)
    up_pre = jnp.dot(section, w_up, preferred_element_type=jnp.float32)
    hidden = (jax.nn.silu(gate_pre) * up_pre).astype(jnp.bfloat16)
    weight_cols = branch_weight
    mix_sum = lax.psum_scatter(
        lax.dot_general(
            weight_cols, pooled, (((0,), (1,)), ((), ())), preferred_element_type=jnp.float32
        ).astype(jnp.bfloat16),
        "tp",
        scatter_dimension=0,
        tiled=True,
    )
    weight_cols = w_down
    exp_sum = lax.psum_scatter(
        lax.dot_general(
            weight_cols, hidden, (((0,), (1,)), ((), ())), preferred_element_type=jnp.float32
        ).astype(jnp.bfloat16),
        "tp",
        scatter_dimension=0,
        tiled=True,
    )
    mix_out = mix_sum.T
    results = exp_sum.reshape(columns, experts_all, capacity)
    returned = lax.all_to_all(results, "ep", split_axis=1, concat_axis=1, tiled=True).reshape(
        columns, experts_all * capacity
    )
    picked = returned[:, slot_index].astype(jnp.float32)
    weighted = picked * route_weights.reshape(-1)[None, :]
    combined = jnp.sum(weighted.reshape(columns, tok_rows, routes.shape[1]), axis=2)
    exp_out = combined.T.astype(jnp.bfloat16)
    return (mix_out, exp_out)


lanes = 128
MESH = pl.DeviceIdType.MESH
f32 = jnp.float32
bf16 = jnp.bfloat16


def fused_kernel(
    x_hbm,
    norm_hbm,
    routes_hbm,
    weights_hbm,
    mix_hbm,
    gain_hbm,
    groups_hbm,
    branch_hbm,
    gate_hbm,
    up_hbm,
    down_hbm,
    mix_out,
    exp_out,
    x_ref,
    norm_ref,
    routes_ref,
    weights_ref,
    mix_ref,
    gain_ref,
    wgu,
    wd,
    wb,
    gw,
    xn,
    sb,
    xg,
    gu,
    hid,
    halo,
    pooled,
    keep_m,
    ps_m,
    pr_m,
    xs_m,
    xr_m,
    keep,
    ps,
    pr,
    xs,
    xr,
    zs,
    zr,
    w_sem,
    i_sem,
    d_send,
    d_recv,
    f_send,
    f_recv,
    p_send,
    p_recv,
    r_send,
    r_recv,
    z_send,
    z_recv,
    m_send,
    m_recv,
    h_sem,
):
    z = lax.axis_index("ep")
    t = lax.axis_index("tp")
    near = t + 1 - 2 * (t % 2)
    across = (t + 2) % 4
    diagonal = (near + 2) % 4
    inner = ((z + 1) // 2) % 2
    peers = [z, z + 1 - 2 * (z % 2), 3 - z, (z + 2) % 4]
    landing = 3 - inner
    slots = [0, 3 - 2 * inner, 2 + inner, 1 + inner]
    homes = [0, 2 - inner, 3, 1 + inner]
    home_of = [
        z,
        inner * peers[1] + (1 - inner) * peers[2],
        peers[3],
        inner * peers[2] + (1 - inner) * peers[1],
    ]
    tokens, width = x_ref.shape
    quarter = width // 4
    cap = xg.shape[2]
    piece = cap // 2
    hid_tiles = gate_hbm.shape[2] // lanes
    rows_mix, channels = mix_ref.shape
    half_mix = rows_mix // 2
    group_count = channels // lanes

    barrier = pltpu.get_barrier_semaphore()
    for k in (1, 2, 3):
        pl.semaphore_signal(barrier, inc=1, device_id={"ep": peers[k]}, device_id_type=MESH)
    for k in (near, across):
        pl.semaphore_signal(barrier, inc=1, device_id={"tp": k}, device_id_type=MESH)

    pairs = (
        (x_hbm, x_ref),
        (norm_hbm, norm_ref),
        (routes_hbm, routes_ref),
        (weights_hbm, weights_ref),
        (mix_hbm, mix_ref),
        (gain_hbm, gain_ref),
    )
    load_i = [pltpu.make_async_copy(src, dst, i_sem.at[i]) for i, (src, dst) in enumerate(pairs)]
    loads = []
    for i in range(2 * hid_tiles):
        src = gate_hbm if i < hid_tiles else up_hbm
        at = (i % hid_tiles) * lanes
        loads.append(
            pltpu.make_async_copy(
                src.at[0, :, pl.ds(at, lanes)],
                wgu.at[i // 2, :, pl.ds((i % 2) * lanes, lanes)],
                w_sem.at[i],
            )
        )
    n0 = 2 * hid_tiles
    load_b = [
        pltpu.make_async_copy(branch_hbm.at[:, pl.ds(k * quarter, quarter)], wb.at[k], w_sem.at[n0 + k])
        for k in range(4)
    ]
    load_d = [
        pltpu.make_async_copy(down_hbm.at[0, :, pl.ds(k * quarter, quarter)], wd.at[k], w_sem.at[n0 + 4 + k])
        for k in range(4)
    ]
    load_g = pltpu.make_async_copy(groups_hbm.at[pl.ds(t * group_count, group_count)], gw, w_sem.at[n0 + 8])
    for c in load_i:
        c.start()

    def remote(src, dst, send, recv, who):
        return pltpu.make_async_remote_copy(
            src_ref=src, dst_ref=dst, send_sem=send, recv_sem=recv, device_id=who, device_id_type=MESH
        )

    for c in load_i[:4]:
        c.wait()
    for c in [load_g] + load_b + loads + load_d:
        c.start()
    floated = x_ref[...].astype(f32)
    scale = lax.rsqrt(jnp.mean(floated * floated, axis=1, keepdims=True) + epsilon)
    xn_val = (floated * scale * norm_ref[...]).astype(bf16)
    for k in range(4):
        xn[k] = xn_val[:, k * quarter : (k + 1) * quarter]
    lane = lax.broadcasted_iota(jnp.int32, (tokens, lanes), 1)
    square = (tokens, tokens)
    diagonal_mask = lax.broadcasted_iota(jnp.int32, square, 0) == lax.broadcasted_iota(jnp.int32, square, 1)

    def column(row):
        spread = jnp.broadcast_to(row, square)
        return jnp.sum(jnp.where(diagonal_mask, spread, jnp.zeros_like(spread)), axis=1, keepdims=True)

    r0 = column(routes_ref[0:1, :].astype(f32)).astype(jnp.int32)
    r1 = column(routes_ref[1:2, :].astype(f32)).astype(jnp.int32)
    w0 = column(weights_ref[0:1, :])
    w1 = column(weights_ref[1:2, :])
    member = ((r0 == lane) | (r1 == lane)).astype(f32)
    above = (
        lax.broadcasted_iota(jnp.int32, (tokens, tokens), 0)
        > lax.broadcasted_iota(jnp.int32, (tokens, tokens), 1)
    ).astype(f32)
    rank = jnp.dot(above.astype(bf16), member.astype(bf16), preferred_element_type=f32)
    slot_lane = lax.broadcasted_iota(jnp.int32, (tokens, cap), 1)
    places = []
    shares = []
    for k in range(4):
        own = jnp.sum(jnp.where(lane == peers[k], rank, 0.0), axis=1, keepdims=True).astype(jnp.int32)
        named = (r0 == peers[k]) | (r1 == peers[k])
        slot = jnp.where(named, own, cap)
        places.append((slot_lane == slot).astype(f32).astype(bf16))
        shares.append(
            jnp.where(r0 == peers[k], w0, 0.0)
            + jnp.where(r1 == peers[k], w1, 0.0)
        )

    def gathered(k, block):
        return lax.dot_general(
            places[k], block, (((0,), (0,)), ((), ())), preferred_element_type=f32
        ).astype(bf16)

    def if_inner(step, k):
        pl.when(inner == 1)(lambda: step(k))

    def if_outer(step, k):
        pl.when(inner == 0)(lambda: step(k))

    own_cols = xn[t]
    sb[0] = gathered(1, own_cols)
    for k in (2, 3):
        sb[k] = gathered(k, own_cols)
    sb[1] = gathered(1, xn[across])
    for c in load_i[4:]:
        c.wait()
    pl.semaphore_wait(barrier, 5)

    def d_z(j, p):
        rows = pl.ds(p * piece, piece)
        q = across if j == 1 else t
        slot = 1 if j < 2 else landing
        at = j if j < 2 else landing
        return remote(
            sb.at[j, rows],
            xg.at[q, slot, rows],
            d_send.at[j, p],
            d_recv.at[at, p],
            {"ep": peers[max(j, 1)]},
        )

    halo_copy = remote(
        mix_ref.at[pl.ds(rows_mix - 16, 16), :], halo, h_sem.at[0], h_sem.at[1], {"ep": (z + 1) % 4}
    )

    @pl.when(z < 3)
    def _():
        halo_copy.start()

    def send_rows(order):
        for j in order:
            for p in range(2):
                d_z(j, p).start()

    if_outer(send_rows, (2, 3, 0, 1))
    if_inner(send_rows, (3, 2, 0, 1))
    for q in range(4):
        xg[q, 0] = gathered(0, xn[q])

    def arrival(at, q, slot, p):
        rows = pl.ds(p * piece, piece)
        return remote(
            sb.at[0, rows], xg.at[q, slot, rows], d_send.at[0, p], d_recv.at[at, p], {"ep": peers[1]}
        )

    def forward(i, q, slot, p):
        rows = pl.ds(p * piece, piece)
        block = xg.at[q, slot, rows]
        return remote(
            block, block, f_send.at[i, slot, p], f_recv.at[i, slot, p], {"tp": across if i == 0 else near}
        )

    def from_z(k):
        if k == 1:
            for p in range(2):
                arrival(0, t, 1, p).wait_recv()
                forward(1, t, 1, p).start()
            for p in range(2):
                arrival(1, across, 1, p).wait_recv()
                forward(2, across, 1, p).start()
            return
        for p in range(2):
            arrival(k, t, k, p).wait_recv()
            forward(0, t, k, p).start()
            forward(1, t, k, p).start()

    def from_x(k):
        for p in range(2):
            forward(0, across, k, p).wait_recv()
            forward(2, across, k, p).start()

    def from_near(k):
        for p in range(2):
            forward(1, near, slots[k], p).wait_recv()
            forward(2, diagonal, slots[k], p).wait_recv()

    def mix_half(h):
        rows = slice(h * half_mix, (h + 1) * half_mix)
        position = z * rows_mix + h * half_mix + lax.broadcasted_iota(jnp.int32, (half_mix, lanes), 0)
        for g in range(group_count):
            cols = slice(g * lanes, (g + 1) * lanes)
            current = mix_ref[rows, cols].astype(f32)
            if h == 0:
                past = halo[:, cols].astype(f32)
            else:
                past = mix_ref[h * half_mix - 16 : h * half_mix, cols].astype(f32)
            total = jnp.concatenate([past, current], axis=0)
            level = g % 4
            for step in range(level + 1):
                total = total + pltpu.roll(total, 1 << step, 0)
            counted = jnp.minimum(position + 1, windows[level]).astype(f32)
            deviation = (total[16:] / counted - current).astype(bf16)
            grouped = jnp.dot(deviation, gw[g], preferred_element_type=f32)
            gain = gain_ref[:, pl.ds(pl.multiple_of(t * channels + g * lanes, lanes), lanes)]
            pooled[rows, cols] = (grouped * gain).astype(bf16)
        for i, q in enumerate((diagonal, near)):
            ps_m[h, i] = jnp.dot(pooled[rows], wb[q], preferred_element_type=f32).astype(bf16)
            m_p(h, i).start()
        for i, q in enumerate((across, t)):
            keep_m[h, i] = jnp.dot(pooled[rows], wb[q], preferred_element_type=f32)

    def m_p(h, i):
        return remote(ps_m.at[h, i], pr_m.at[h, i], m_send.at[h, i], m_recv.at[h, i], {"tp": near})

    def m_x(h):
        return remote(xs_m.at[h], xr_m.at[h], m_send.at[h, 2], m_recv.at[h, 2], {"tp": across})

    def send_mix(h):
        m_p(h, 0).wait_recv()
        xs_m[h] = (keep_m[h, 0] + pr_m[h, 0].astype(f32)).astype(bf16)
        m_x(h).start()

    def finish_mix(h):
        m_p(h, 1).wait_recv()
        m_x(h).wait_recv()
        total = keep_m[h, 1] + pr_m[h, 1].astype(f32) + xr_m[h].astype(f32)
        mix_out[h * half_mix : (h + 1) * half_mix] = total.astype(bf16)

    def expand(k, first, last):
        for n in range(first, last):
            if k == 0:
                loads[2 * n].wait()
                loads[2 * n + 1].wait()
            total = None
            for q in range(4):
                part = jnp.dot(
                    xg[q, slots[k]], wgu[n, q * quarter : (q + 1) * quarter, :], preferred_element_type=f32
                )
                total = part if total is None else total + part
            gu[n] = total

    def activate(k):
        for i in range(hid_tiles):
            m = hid_tiles + i
            gate = gu[i // 2, :, (i % 2) * lanes : (i % 2 + 1) * lanes]
            up = gu[m // 2, :, (m % 2) * lanes : (m % 2 + 1) * lanes]
            hid[k, :, i * lanes : (i + 1) * lanes] = (gate / (1.0 + jnp.exp(-gate)) * up).astype(bf16)

    def r_p(i, k):
        return remote(ps.at[i, k], pr.at[i, k], p_send.at[i, k], p_recv.at[i, k], {"tp": near})

    def r_x(k, p):
        rows = pl.ds(p * piece, piece)
        return remote(xs.at[k, rows], xr.at[k, rows], r_send.at[k, p], r_recv.at[k, p], {"tp": across})

    def r_z(k, p):
        rows = pl.ds(p * piece, piece)
        return remote(
            zs.at[k, rows],
            zr.at[homes[k], rows],
            z_send.at[k, p],
            z_recv.at[homes[k], p],
            {"ep": home_of[k]},
        )

    def project(k):
        for i, q in enumerate((diagonal, across, near, t)):
            part = jnp.dot(hid[k], wd[q], preferred_element_type=f32)
            if i % 2 == 0:
                ps[i // 2, k] = part.astype(bf16)
                r_p(i // 2, k).start()
            else:
                keep[i // 2, k] = part

    def send_x(k):
        r_p(0, k).wait_recv()
        for p in range(2):
            rows = slice(p * piece, (p + 1) * piece)
            xs[k, rows] = (keep[0, k, rows] + pr[0, k, rows].astype(f32)).astype(bf16)
            r_x(k, p).start()

    def send_z(k):
        r_p(1, k).wait_recv()
        for p in range(2):
            rows = slice(p * piece, (p + 1) * piece)
            r_x(k, p).wait_recv()
            zs[k, rows] = (keep[1, k, rows] + pr[1, k, rows].astype(f32) + xr[k, rows].astype(f32)).astype(bf16)
            if k > 0:
                r_z(k, p).start()

    def share(k):
        block = zs[0] if k == 0 else zr[k]
        return shares[k] * jnp.dot(places[k], block, preferred_element_type=f32)

    def returned(k):
        for p in range(2):
            rows = pl.ds(p * piece, piece)
            remote(
                zs.at[k, rows], zr.at[k, rows], z_send.at[k, p], z_recv.at[k, p], {"ep": peers[k]}
            ).wait_recv()

    half = hid_tiles // 2
    load_g.wait()
    for c in load_b:
        c.wait()
    mix_half(1)
    expand(0, 0, half)
    send_mix(1)
    expand(0, half, hid_tiles)
    activate(0)
    for c in load_d:
        c.wait()
    project(0)
    if_outer(from_z, 3)

    @pl.when(z == 0)
    def _():
        halo[...] = jnp.zeros_like(halo)

    @pl.when(z > 0)
    def _():
        halo_copy.wait_recv()

    mix_half(0)
    if_inner(from_z, 3)
    if_inner(send_x, 0)
    if_outer(from_z, 2)
    if_outer(send_x, 0)
    if_outer(from_x, 3)
    from_z(1)
    if_inner(from_z, 2)
    if_inner(from_x, 3)
    from_near(1)
    expand(1, 0, hid_tiles)
    activate(1)
    if_outer(from_x, 2)
    project(1)
    from_near(2)
    expand(2, 0, 2)
    send_x(1)
    expand(2, 2, hid_tiles)
    activate(2)
    if_inner(from_x, 2)
    project(2)
    from_near(3)
    expand(3, 0, 2)
    send_x(2)
    expand(3, 2, hid_tiles)
    activate(3)
    send_z(1)
    project(3)
    send_x(3)
    send_z(2)
    send_z(0)
    send_mix(0)
    finish_mix(1)
    result = share(0)
    send_z(3)
    returned(3)
    result = result + share(3)
    finish_mix(0)
    for k in (1, 2):
        returned(k)
        result = result + share(k)
    exp_out[...] = result.astype(bf16)

    @pl.when(z < 3)
    def _():
        halo_copy.wait_send()

    for k in (1, 2, 3):
        for p in range(2):
            if k > 1:
                forward(0, t, k, p).wait_send()
            forward(1, t, k, p).wait_send()
            forward(2, across, k, p).wait_send()
            r_z(k, p).wait_send()
    for k in range(4):
        for p in range(2):
            d_z(k, p).wait_send()
            r_x(k, p).wait_send()
            r_p(p, k).wait_send()
    for h in range(2):
        m_p(h, 0).wait_send()
        m_p(h, 1).wait_send()
        m_x(h).wait_send()


def store_kernel(mix_ref, exp_ref, mix_hbm, exp_hbm, sem):
    stores = [
        pltpu.make_async_copy(mix_ref, mix_hbm, sem.at[0]),
        pltpu.make_async_copy(exp_ref, exp_hbm, sem.at[1]),
    ]
    for c in stores:
        c.start()
    for c in stores:
        c.wait()


def fused(
    mix_input,
    group_weight,
    pool_gain,
    branch_weight,
    exp_input,
    norm_gain,
    routes,
    route_weights,
    gate_weight,
    up_weight,
    down_weight,
):
    tokens, width = exp_input.shape
    rows_mix, channels = mix_input.shape
    hidden = gate_weight.shape[2]
    quarter = width // 4
    cap = 3 * tokens // 4
    hid_tiles = hidden // lanes
    half_mix = rows_mix // 2
    vmem = pl.BlockSpec(memory_space=pltpu.VMEM)
    anywhere = pl.BlockSpec(memory_space=pl.ANY)
    dma = pltpu.SemaphoreType.DMA
    mix_out, exp_out = pl.pallas_call(
        fused_kernel,
        out_shape=(
            pltpu.VMEM((rows_mix, quarter), bf16),
            pltpu.VMEM((tokens, quarter), bf16),
        ),
        in_specs=[anywhere] * 11,
        out_specs=(vmem, vmem),
        scratch_shapes=[
            pltpu.VMEM((tokens, width), bf16),
            pltpu.VMEM((1, width), f32),
            pltpu.VMEM((2, tokens), jnp.int32),
            pltpu.VMEM((2, tokens), f32),
            pltpu.VMEM((rows_mix, channels), bf16),
            pltpu.VMEM((1, 4 * channels), f32),
            pltpu.VMEM((hid_tiles, width, 2 * lanes), bf16),
            pltpu.VMEM((4, hidden, quarter), bf16),
            pltpu.VMEM((4, channels, quarter), bf16),
            pltpu.VMEM((channels // lanes, lanes, lanes), bf16),
            pltpu.VMEM((4, tokens, quarter), bf16),
            pltpu.VMEM((4, cap, quarter), bf16),
            pltpu.VMEM((4, 4, cap, quarter), bf16),
            pltpu.VMEM((hid_tiles, cap, 2 * lanes), f32),
            pltpu.VMEM((4, cap, hidden), bf16),
            pltpu.VMEM((16, channels), bf16),
            pltpu.VMEM((rows_mix, channels), bf16),
            pltpu.VMEM((2, 2, half_mix, quarter), f32),
            pltpu.VMEM((2, 2, half_mix, quarter), bf16),
            pltpu.VMEM((2, 2, half_mix, quarter), bf16),
            pltpu.VMEM((2, half_mix, quarter), bf16),
            pltpu.VMEM((2, half_mix, quarter), bf16),
            pltpu.VMEM((2, 4, cap, quarter), f32),
            pltpu.VMEM((2, 4, cap, quarter), bf16),
            pltpu.VMEM((2, 4, cap, quarter), bf16),
            pltpu.VMEM((4, cap, quarter), bf16),
            pltpu.VMEM((4, cap, quarter), bf16),
            pltpu.VMEM((4, cap, quarter), bf16),
            pltpu.VMEM((4, cap, quarter), bf16),
            dma((2 * hid_tiles + 9,)),
            dma((6,)),
            dma((4, 2)),
            dma((4, 2)),
            dma((3, 4, 2)),
            dma((3, 4, 2)),
            dma((2, 4)),
            dma((2, 4)),
            dma((4, 2)),
            dma((4, 2)),
            dma((4, 2)),
            dma((4, 2)),
            dma((2, 3)),
            dma((2, 3)),
            dma((2,)),
        ],
        compiler_params=pltpu.CompilerParams(
            collective_id=0, has_side_effects=True, vmem_limit_bytes=56 << 20
        ),
    )(
        exp_input,
        norm_gain.reshape(1, -1),
        routes.T,
        route_weights.T,
        mix_input,
        pool_gain.reshape(1, -1),
        group_weight,
        branch_weight,
        gate_weight,
        up_weight,
        down_weight,
    )
    return pl.pallas_call(
        store_kernel,
        out_shape=(
            jax.ShapeDtypeStruct((rows_mix, quarter), bf16),
            jax.ShapeDtypeStruct((tokens, quarter), bf16),
        ),
        in_specs=[vmem] * 2,
        out_specs=(anywhere, anywhere),
        scratch_shapes=[dma((2,))],
    )(
        pltpu.with_memory_space_constraint(mix_out, pltpu.VMEM),
        pltpu.with_memory_space_constraint(exp_out, pltpu.VMEM),
    )


def fits(mesh, args):
    mix, group, _, _, tok, _, routes, _, gate, _, _ = args
    ep, tp, grp = (mesh.shape[k] for k in ("ep", "tp", "grp"))
    if ep != 4 or tp != 4 or routes.shape[1] != 2 or gate.shape[0] != ep:
        return False
    rows, channels = mix.shape[0] // (grp * ep), mix.shape[1] // tp
    tokens, quarter = tok.shape[0] // (grp * ep), tok.shape[1] // tp
    return (
        group.shape[1] == lanes
        and channels % (4 * lanes) == 0
        and channels == quarter
        and rows % 32 == 0
        and tokens % 64 == 0
        and gate.shape[2] % (tp * lanes) == 0
        and gate.shape[1] * gate.shape[2] <= 1 << 23
        and rows <= 512
        and tokens <= 256
    )


def solution(mesh):
    def run(*args):
        body = fused if fits(mesh, args) else on_device
        return jax.shard_map(
            body,
            mesh=mesh,
            in_specs=(
                P(("grp", "ep"), "tp"),
                P(),
                P(),
                P("tp", None),
                P(("grp", "ep"), None),
                P(),
                P(("grp", "ep"), None),
                P(("grp", "ep"), None),
                P("ep", None, "tp"),
                P("ep", None, "tp"),
                P("ep", "tp", None),
            ),
            out_specs=(P(("grp", "ep"), "tp"), P(("grp", "ep"), "tp")),
            check_vma=False,
        )(*args)

    return run
```

```python
import functools

import jax
import jax.numpy as jnp
from jax import lax
from jax.experimental import pallas as pl
from jax.experimental.pallas import tpu as pltpu
from jax.sharding import PartitionSpec as P

windows = (2, 4, 8, 16)
epsilon = 1e-06


def shifted(block, axis, distance):
    devices = range(lax.axis_size(axis))
    route = [(i - distance, i) for i in devices if i - distance in devices]
    return lax.ppermute(block, axis, route)


def trailing_sums(extended, rows):
    span_two = extended[1:] + extended[:-1]
    span_four = span_two[2:] + span_two[:-2]
    span_eight = span_four[4:] + span_four[:-4]
    span_sixteen = span_eight[8:] + span_eight[:-8]
    return [span_two[-rows:], span_four[-rows:], span_eight[-rows:], span_sixteen]


def pooled_deviation(extended, positions, group_ids, group_width, rows):
    sums = trailing_sums(extended, rows)
    current = extended[-rows:]
    window_id = jnp.repeat(group_ids % 4, group_width)
    result = jnp.zeros_like(current)
    for window_level, window_len in enumerate(windows):
        counted = jnp.minimum(positions + 1, window_len).astype(jnp.float32)[:, None]
        result = jnp.where(
            window_id[None, :] == window_level, sums[window_level] / counted - current, result
        )
    return result


def on_device(
    mix_input,
    group_weight,
    pool_gain,
    branch_weight,
    exp_input,
    norm_gain,
    routes,
    route_weights,
    gate_weight,
    up_weight,
    down_weight,
):
    tp_rank = lax.axis_index("tp")
    ep_rank = lax.axis_index("ep")
    rows_mix, channels = mix_input.shape
    group_width = group_weight.shape[1]
    group_count = channels // group_width
    first_group = tp_rank * group_count
    last_rows = mix_input[rows_mix - 15 :]
    before = shifted(last_rows, "ep", 1)
    extended = jnp.concatenate([before, mix_input], axis=0).astype(jnp.float32)
    positions = ep_rank * rows_mix + jnp.arange(rows_mix, dtype=jnp.int32)
    group_ids = first_group + jnp.arange(group_count, dtype=jnp.int32)
    deviation = pooled_deviation(extended, positions, group_ids, group_width, rows_mix).astype(
        jnp.bfloat16
    )
    own_groups = lax.dynamic_slice_in_dim(group_weight, first_group, group_count, 0)
    grouped = jnp.einsum(
        "rgc,gcd->rgd",
        deviation.reshape(rows_mix, group_count, group_width),
        own_groups,
        preferred_element_type=jnp.float32,
    ).reshape(rows_mix, channels)
    own_gain = lax.dynamic_slice_in_dim(pool_gain, first_group * group_width, channels, 0)
    pooled = (grouped * own_gain).astype(jnp.bfloat16)
    tok_rows, width = exp_input.shape
    columns = width // lax.axis_size("tp")
    experts_all = lax.axis_size("ep")
    capacity = 3 * tok_rows // experts_all
    floated = exp_input.astype(jnp.float32)
    normed = (
        floated
        * lax.rsqrt(jnp.mean(floated * floated, axis=1, keepdims=True) + epsilon)
        * norm_gain
    ).astype(jnp.bfloat16)
    flat_expert = routes.reshape(-1)
    assignments = flat_expert.shape[0]
    onehot = (flat_expert[:, None] == jnp.arange(experts_all, dtype=jnp.int32)[None, :]).astype(
        jnp.int32
    )
    slot_rank = jnp.sum((jnp.cumsum(onehot, axis=0) - onehot) * onehot, axis=1)
    slot_index = flat_expert * capacity + slot_rank
    token_of = jnp.arange(assignments, dtype=jnp.int32) // routes.shape[1]
    slot_token = (
        jnp.full((experts_all * capacity,), tok_rows, jnp.int32).at[slot_index].set(token_of)
    )
    padded = jnp.concatenate([normed, jnp.zeros((1, width), jnp.bfloat16)], axis=0)
    w_gate = gate_weight[0]
    w_up = up_weight[0]
    w_down = down_weight[0]
    arrived_rows = experts_all * capacity
    own_columns = lax.dynamic_slice_in_dim(padded, tp_rank * columns, columns, 1)
    outgoing = own_columns[slot_token].reshape(experts_all, capacity, columns)
    arrived = lax.all_to_all(outgoing, "ep", split_axis=0, concat_axis=0, tiled=True).reshape(
        arrived_rows, columns
    )
    section = lax.all_gather(arrived, "tp", axis=1, tiled=True)
    gate_pre = jnp.dot(section, w_gate, preferred_element_type=jnp.float32)
    up_pre = jnp.dot(section, w_up, preferred_element_type=jnp.float32)
    hidden = (jax.nn.silu(gate_pre) * up_pre).astype(jnp.bfloat16)
    weight_cols = branch_weight
    mix_sum = lax.psum_scatter(
        lax.dot_general(
            weight_cols, pooled, (((0,), (1,)), ((), ())), preferred_element_type=jnp.float32
        ).astype(jnp.bfloat16),
        "tp",
        scatter_dimension=0,
        tiled=True,
    )
    weight_cols = w_down
    exp_sum = lax.psum_scatter(
        lax.dot_general(
            weight_cols, hidden, (((0,), (1,)), ((), ())), preferred_element_type=jnp.float32
        ).astype(jnp.bfloat16),
        "tp",
        scatter_dimension=0,
        tiled=True,
    )
    mix_out = mix_sum.T
    results = exp_sum.reshape(columns, experts_all, capacity)
    returned = lax.all_to_all(results, "ep", split_axis=1, concat_axis=1, tiled=True).reshape(
        columns, experts_all * capacity
    )
    picked = returned[:, slot_index].astype(jnp.float32)
    weighted = picked * route_weights.reshape(-1)[None, :]
    combined = jnp.sum(weighted.reshape(columns, tok_rows, routes.shape[1]), axis=2)
    exp_out = combined.T.astype(jnp.bfloat16)
    return (mix_out, exp_out)


lanes = 128
MESH = pl.DeviceIdType.MESH
f32 = jnp.float32
bf16 = jnp.bfloat16


def fused_kernel(
    x_hbm,
    norm_hbm,
    routes_hbm,
    weights_hbm,
    mix_hbm,
    gain_hbm,
    groups_hbm,
    branch_hbm,
    gate_hbm,
    up_hbm,
    down_hbm,
    mix_out,
    exp_out,
    x_ref,
    norm_ref,
    routes_ref,
    weights_ref,
    mix_ref,
    gain_ref,
    wgu,
    wd,
    wb,
    gw,
    xn,
    sb,
    xg,
    gu,
    hid,
    halo,
    pooled,
    keep_m,
    ps_m,
    pr_m,
    xs_m,
    xr_m,
    keep,
    ps,
    pr,
    xs,
    xr,
    zs,
    zr,
    w_sem,
    i_sem,
    d_send,
    d_recv,
    f_send,
    f_recv,
    p_send,
    p_recv,
    r_send,
    r_recv,
    z_send,
    z_recv,
    m_send,
    m_recv,
    h_sem,
):
    z = lax.axis_index("ep")
    t = lax.axis_index("tp")
    near = t + 1 - 2 * (t % 2)
    across = (t + 2) % 4
    diagonal = (near + 2) % 4
    inner = ((z + 1) // 2) % 2
    peers = [z, z + 1 - 2 * (z % 2), 3 - z, (z + 2) % 4]
    landing = 3 - inner
    slots = [0, 3, 2 - inner, 1 + inner]
    homes = [0, 2 + inner, 3 - 2 * inner, 1 + inner]
    home_of = [
        z,
        inner * peers[3] + (1 - inner) * peers[2],
        inner * peers[1] + (1 - inner) * peers[3],
        inner * peers[2] + (1 - inner) * peers[1],
    ]
    second = inner * across + (1 - inner) * near
    third = inner * near + (1 - inner) * across
    early = [None, (t, near), (t, second), (t, third)]
    late = [None, (across, diagonal), (third, diagonal), (second, diagonal)]
    tokens, width = x_ref.shape
    quarter = width // 4
    cap = xg.shape[2]
    piece = cap // 2
    hid_tiles = gate_hbm.shape[2] // lanes
    rows_mix, channels = mix_ref.shape
    half_mix = rows_mix // 2
    group_count = channels // lanes

    barrier = pltpu.get_barrier_semaphore()
    for k in (1, 2, 3):
        pl.semaphore_signal(barrier, inc=1, device_id={"ep": peers[k]}, device_id_type=MESH)
    for k in (near, across):
        pl.semaphore_signal(barrier, inc=1, device_id={"tp": k}, device_id_type=MESH)

    pairs = (
        (routes_hbm, routes_ref),
        (weights_hbm, weights_ref),
        (x_hbm, x_ref),
        (norm_hbm, norm_ref),
        (mix_hbm, mix_ref),
        (gain_hbm, gain_ref),
    )
    load_i = [pltpu.make_async_copy(src, dst, i_sem.at[i]) for i, (src, dst) in enumerate(pairs)]
    loads = []
    for i in range(2 * hid_tiles):
        src = gate_hbm if i < hid_tiles else up_hbm
        at = (i % hid_tiles) * lanes
        loads.append(
            pltpu.make_async_copy(
                src.at[0, :, pl.ds(at, lanes)],
                wgu.at[i // 2, :, pl.ds((i % 2) * lanes, lanes)],
                w_sem.at[i],
            )
        )
    n0 = 2 * hid_tiles
    load_b = [
        pltpu.make_async_copy(branch_hbm.at[:, pl.ds(k * quarter, quarter)], wb.at[k], w_sem.at[n0 + k])
        for k in range(4)
    ]
    load_d = [
        pltpu.make_async_copy(down_hbm.at[0, :, pl.ds(k * quarter, quarter)], wd.at[k], w_sem.at[n0 + 4 + k])
        for k in range(4)
    ]
    load_g = pltpu.make_async_copy(groups_hbm.at[pl.ds(t * group_count, group_count)], gw, w_sem.at[n0 + 8])
    for c in load_i:
        c.start()

    def remote(src, dst, send, recv, who):
        return pltpu.make_async_remote_copy(
            src_ref=src, dst_ref=dst, send_sem=send, recv_sem=recv, device_id=who, device_id_type=MESH
        )

    for c in load_i[:2]:
        c.wait()
    lane = lax.broadcasted_iota(jnp.int32, (tokens, lanes), 1)
    square = (tokens, tokens)
    diagonal_mask = lax.broadcasted_iota(jnp.int32, square, 0) == lax.broadcasted_iota(jnp.int32, square, 1)

    def column(row):
        spread = jnp.broadcast_to(row, square)
        return jnp.sum(jnp.where(diagonal_mask, spread, jnp.zeros_like(spread)), axis=1, keepdims=True)

    r0 = column(routes_ref[0:1, :].astype(f32)).astype(jnp.int32)
    r1 = column(routes_ref[1:2, :].astype(f32)).astype(jnp.int32)
    w0 = column(weights_ref[0:1, :])
    w1 = column(weights_ref[1:2, :])
    member = ((r0 == lane) | (r1 == lane)).astype(f32)
    above = (
        lax.broadcasted_iota(jnp.int32, (tokens, tokens), 0)
        > lax.broadcasted_iota(jnp.int32, (tokens, tokens), 1)
    ).astype(f32)
    rank = jnp.dot(above.astype(bf16), member.astype(bf16), preferred_element_type=f32)
    slot_lane = lax.broadcasted_iota(jnp.int32, (tokens, cap), 1)
    places = []
    shares = []
    for k in range(4):
        own = jnp.sum(jnp.where(lane == peers[k], rank, 0.0), axis=1, keepdims=True).astype(jnp.int32)
        named = (r0 == peers[k]) | (r1 == peers[k])
        slot = jnp.where(named, own, cap)
        places.append((slot_lane == slot).astype(f32).astype(bf16))
        shares.append(
            jnp.where(r0 == peers[k], w0, 0.0)
            + jnp.where(r1 == peers[k], w1, 0.0)
        )

    for c in load_i[2:4]:
        c.wait()
    for c in [load_g] + load_b + loads + load_d:
        c.start()
    floated = x_ref[...].astype(f32)
    scale = lax.rsqrt(jnp.mean(floated * floated, axis=1, keepdims=True) + epsilon)
    xn_val = (floated * scale * norm_ref[...]).astype(bf16)
    for k in range(4):
        xn[k] = xn_val[:, k * quarter : (k + 1) * quarter]

    def gathered(k, block):
        return lax.dot_general(
            places[k], block, (((0,), (0,)), ((), ())), preferred_element_type=f32
        ).astype(bf16)

    def if_inner(step, k):
        pl.when(inner == 1)(lambda: step(k))

    def if_outer(step, k):
        pl.when(inner == 0)(lambda: step(k))

    own_cols = xn[t]
    for k in (2, 3):
        sb[k] = gathered(k, own_cols)
    for c in load_i[4:]:
        c.wait()
    pl.semaphore_wait(barrier, 5)

    def d_z(j, p):
        rows = pl.ds(p * piece, piece)
        q = across if j == 1 else t
        slot = 1 if j < 2 else landing
        at = j if j < 2 else landing
        return remote(
            sb.at[j, rows],
            xg.at[q, slot, rows],
            d_send.at[j, p],
            d_recv.at[at, p],
            {"ep": peers[max(j, 1)]},
        )

    halo_copy = remote(
        mix_ref.at[pl.ds(rows_mix - 16, 16), :], halo, h_sem.at[0], h_sem.at[1], {"ep": (z + 1) % 4}
    )

    @pl.when(z < 3)
    def _():
        halo_copy.start()

    def send_rows(order):
        for j in order:
            for p in range(2):
                d_z(j, p).start()

    if_outer(send_rows, (2, 3))
    if_inner(send_rows, (3, 2))
    sb[0] = gathered(1, own_cols)
    sb[1] = gathered(1, xn[across])
    send_rows((0, 1))
    for q in range(4):
        xg[q, 0] = gathered(0, xn[q])

    def arrival(at, q, slot, p):
        rows = pl.ds(p * piece, piece)
        return remote(
            sb.at[0, rows], xg.at[q, slot, rows], d_send.at[0, p], d_recv.at[at, p], {"ep": peers[1]}
        )

    def forward(i, q, slot, p):
        rows = pl.ds(p * piece, piece)
        block = xg.at[q, slot, rows]
        return remote(
            block, block, f_send.at[i, slot, p], f_recv.at[i, slot, p], {"tp": across if i == 0 else near}
        )

    def from_z(k):
        if k == 1:
            for p in range(2):
                arrival(0, t, 1, p).wait_recv()
                forward(1, t, 1, p).start()
            for p in range(2):
                arrival(1, across, 1, p).wait_recv()
                forward(2, across, 1, p).start()
            return
        for p in range(2):
            arrival(k, t, k, p).wait_recv()
            forward(0, t, k, p).start()
            forward(1, t, k, p).start()

    def from_x(k):
        for p in range(2):
            forward(0, across, k, p).wait_recv()
            forward(2, across, k, p).start()

    def near_own(k):
        for p in range(2):
            forward(1, near, k, p).wait_recv()

    def near_other(k):
        for p in range(2):
            forward(2, diagonal, k, p).wait_recv()

    def mix_half(h):
        rows = slice(h * half_mix, (h + 1) * half_mix)
        position = z * rows_mix + h * half_mix + lax.broadcasted_iota(jnp.int32, (half_mix, lanes), 0)
        for g in range(group_count):
            cols = slice(g * lanes, (g + 1) * lanes)
            current = mix_ref[rows, cols].astype(f32)
            if h == 0:
                past = halo[:, cols].astype(f32)
            else:
                past = mix_ref[h * half_mix - 16 : h * half_mix, cols].astype(f32)
            total = jnp.concatenate([past, current], axis=0)
            level = g % 4
            for step in range(level + 1):
                total = total + pltpu.roll(total, 1 << step, 0)
            counted = jnp.minimum(position + 1, windows[level]).astype(f32)
            deviation = (total[16:] / counted - current).astype(bf16)
            grouped = jnp.dot(deviation, gw[g], preferred_element_type=f32)
            gain = gain_ref[:, pl.ds(pl.multiple_of(t * channels + g * lanes, lanes), lanes)]
            pooled[rows, cols] = (grouped * gain).astype(bf16)
        for i, q in enumerate((diagonal, near)):
            ps_m[h, i] = jnp.dot(pooled[rows], wb[q], preferred_element_type=f32).astype(bf16)
        for i, q in enumerate((across, t)):
            keep_m[h, i] = jnp.dot(pooled[rows], wb[q], preferred_element_type=f32)
        for i in range(2):
            m_p(h, i).start()

    def m_p(h, i):
        return remote(ps_m.at[h, i], pr_m.at[h, i], m_send.at[h, i], m_recv.at[h, i], {"tp": near})

    def m_x(h):
        return remote(xs_m.at[h], xr_m.at[h], m_send.at[h, 2], m_recv.at[h, 2], {"tp": across})

    def send_mix(h):
        m_p(h, 0).wait_recv()
        xs_m[h] = (keep_m[h, 0] + pr_m[h, 0].astype(f32)).astype(bf16)
        m_x(h).start()

    def finish_mix(h):
        m_p(h, 1).wait_recv()
        m_x(h).wait_recv()
        total = keep_m[h, 1] + pr_m[h, 1].astype(f32) + xr_m[h].astype(f32)
        mix_out[h * half_mix : (h + 1) * half_mix] = total.astype(bf16)

    def expand(k, blocks, first, last):
        for n in range(first, last):
            if k == 0:
                loads[2 * n].wait()
                loads[2 * n + 1].wait()
            total = None if blocks is None or blocks is early[k] else gu[k, n]
            for q in range(4) if blocks is None else blocks:
                rows = pl.ds(q * quarter if blocks is None else pl.multiple_of(q * quarter, quarter), quarter)
                part = jnp.dot(xg[q, slots[k]], wgu[n, rows, :], preferred_element_type=f32)
                total = part if total is None else total + part
            gu[k, n] = total

    def activate(k):
        for i in range(hid_tiles):
            m = hid_tiles + i
            gate = gu[k, i // 2, :, (i % 2) * lanes : (i % 2 + 1) * lanes]
            up = gu[k, m // 2, :, (m % 2) * lanes : (m % 2 + 1) * lanes]
            hid[k, :, i * lanes : (i + 1) * lanes] = (gate / (1.0 + jnp.exp(-gate)) * up).astype(bf16)

    def r_p(i, k):
        return remote(ps.at[i, k], pr.at[i, k], p_send.at[i, k], p_recv.at[i, k], {"tp": near})

    def r_x(k, p):
        rows = pl.ds(p * piece, piece)
        return remote(xs.at[k, rows], xr.at[k, rows], r_send.at[k, p], r_recv.at[k, p], {"tp": across})

    def r_z(k, p):
        rows = pl.ds(p * piece, piece)
        return remote(
            zs.at[k, rows],
            zr.at[homes[k], rows],
            z_send.at[k, p],
            z_recv.at[homes[k], p],
            {"ep": home_of[k]},
        )

    def project(k):
        for i, q in enumerate((diagonal, near, across, t)):
            part = jnp.dot(hid[k], wd[q], preferred_element_type=f32)
            if i < 2:
                ps[i, k] = part.astype(bf16)
            else:
                keep[i - 2, k] = part
            if i == 0:
                r_p(0, k).start()
        r_p(1, k).start()

    def send_x(k):
        r_p(0, k).wait_recv()
        for p in range(2):
            rows = slice(p * piece, (p + 1) * piece)
            xs[k, rows] = (keep[0, k, rows] + pr[0, k, rows].astype(f32)).astype(bf16)
            r_x(k, p).start()

    def send_z(k):
        r_p(1, k).wait_recv()
        for p in range(2):
            rows = slice(p * piece, (p + 1) * piece)
            r_x(k, p).wait_recv()
            zs[k, rows] = (keep[1, k, rows] + pr[1, k, rows].astype(f32) + xr[k, rows].astype(f32)).astype(bf16)
            if k > 0:
                r_z(k, p).start()

    def share(k):
        block = zs[0] if k == 0 else zr[k]
        return shares[k] * jnp.dot(places[k], block, preferred_element_type=f32)

    def returned(k):
        for p in range(2):
            rows = pl.ds(p * piece, piece)
            remote(
                zs.at[k, rows], zr.at[k, rows], z_send.at[k, p], z_recv.at[k, p], {"ep": peers[k]}
            ).wait_recv()

    half = hid_tiles // 2
    load_g.wait()
    for c in load_b:
        c.wait()
    mix_half(1)
    expand(0, None, 0, half)
    send_mix(1)
    expand(0, None, half, hid_tiles)
    activate(0)
    for c in load_d:
        c.wait()
    project(0)
    if_outer(from_z, 3)

    @pl.when(z == 0)
    def _():
        halo[...] = jnp.zeros_like(halo)

    @pl.when(z > 0)
    def _():
        halo_copy.wait_recv()

    mix_half(0)
    if_inner(from_z, 3)
    near_own(3)
    expand(1, early[1], 0, hid_tiles)
    if_outer(from_z, 2)
    if_outer(from_x, 3)
    from_z(1)
    if_inner(from_z, 2)
    if_inner(from_x, 3)
    expand(1, late[1][:1], 0, hid_tiles)
    send_x(0)
    if_outer(near_own, 2)
    expand(2, early[2], 0, hid_tiles)
    near_other(3)
    expand(1, late[1][1:], 0, hid_tiles)
    activate(1)
    project(1)
    if_outer(from_x, 2)
    if_inner(near_own, 2)
    expand(3, early[3], 0, hid_tiles)
    send_x(1)
    if_inner(near_own, 1)
    if_inner(near_other, 1)
    if_outer(near_other, 2)
    expand(2, late[2], 0, hid_tiles)
    activate(2)
    if_inner(from_x, 2)
    project(2)
    if_outer(near_own, 1)
    if_outer(near_other, 1)
    if_inner(near_other, 2)
    expand(3, late[3], 0, half)
    send_x(2)
    expand(3, late[3], half, hid_tiles)
    activate(3)
    if_outer(send_z, 1)
    project(3)
    if_inner(send_z, 1)
    send_x(3)
    send_z(2)
    send_z(0)
    send_mix(0)
    finish_mix(1)
    result = share(0)
    send_z(3)
    returned(3)
    result = result + share(3)
    finish_mix(0)
    for k in (1, 2):
        returned(k)
        result = result + share(k)
    exp_out[...] = result.astype(bf16)

    @pl.when(z < 3)
    def _():
        halo_copy.wait_send()

    for k in (1, 2, 3):
        for p in range(2):
            if k > 1:
                forward(0, t, k, p).wait_send()
            forward(1, t, k, p).wait_send()
            forward(2, across, k, p).wait_send()
            r_z(k, p).wait_send()
    for k in range(4):
        for p in range(2):
            d_z(k, p).wait_send()
            r_x(k, p).wait_send()
            r_p(p, k).wait_send()
    for h in range(2):
        m_p(h, 0).wait_send()
        m_p(h, 1).wait_send()
        m_x(h).wait_send()


def store_kernel(mix_ref, exp_ref, mix_hbm, exp_hbm, sem):
    stores = [
        pltpu.make_async_copy(mix_ref, mix_hbm, sem.at[0]),
        pltpu.make_async_copy(exp_ref, exp_hbm, sem.at[1]),
    ]
    for c in stores:
        c.start()
    for c in stores:
        c.wait()


def fused(
    mix_input,
    group_weight,
    pool_gain,
    branch_weight,
    exp_input,
    norm_gain,
    routes,
    route_weights,
    gate_weight,
    up_weight,
    down_weight,
):
    tokens, width = exp_input.shape
    rows_mix, channels = mix_input.shape
    hidden = gate_weight.shape[2]
    quarter = width // 4
    cap = 3 * tokens // 4
    hid_tiles = hidden // lanes
    half_mix = rows_mix // 2
    vmem = pl.BlockSpec(memory_space=pltpu.VMEM)
    anywhere = pl.BlockSpec(memory_space=pl.ANY)
    dma = pltpu.SemaphoreType.DMA
    mix_out, exp_out = pl.pallas_call(
        fused_kernel,
        out_shape=(
            pltpu.VMEM((rows_mix, quarter), bf16),
            pltpu.VMEM((tokens, quarter), bf16),
        ),
        in_specs=[anywhere] * 11,
        out_specs=(vmem, vmem),
        scratch_shapes=[
            pltpu.VMEM((tokens, width), bf16),
            pltpu.VMEM((1, width), f32),
            pltpu.VMEM((2, tokens), jnp.int32),
            pltpu.VMEM((2, tokens), f32),
            pltpu.VMEM((rows_mix, channels), bf16),
            pltpu.VMEM((1, 4 * channels), f32),
            pltpu.VMEM((hid_tiles, width, 2 * lanes), bf16),
            pltpu.VMEM((4, hidden, quarter), bf16),
            pltpu.VMEM((4, channels, quarter), bf16),
            pltpu.VMEM((channels // lanes, lanes, lanes), bf16),
            pltpu.VMEM((4, tokens, quarter), bf16),
            pltpu.VMEM((4, cap, quarter), bf16),
            pltpu.VMEM((4, 4, cap, quarter), bf16),
            pltpu.VMEM((4, hid_tiles, cap, 2 * lanes), f32),
            pltpu.VMEM((4, cap, hidden), bf16),
            pltpu.VMEM((16, channels), bf16),
            pltpu.VMEM((rows_mix, channels), bf16),
            pltpu.VMEM((2, 2, half_mix, quarter), f32),
            pltpu.VMEM((2, 2, half_mix, quarter), bf16),
            pltpu.VMEM((2, 2, half_mix, quarter), bf16),
            pltpu.VMEM((2, half_mix, quarter), bf16),
            pltpu.VMEM((2, half_mix, quarter), bf16),
            pltpu.VMEM((2, 4, cap, quarter), f32),
            pltpu.VMEM((2, 4, cap, quarter), bf16),
            pltpu.VMEM((2, 4, cap, quarter), bf16),
            pltpu.VMEM((4, cap, quarter), bf16),
            pltpu.VMEM((4, cap, quarter), bf16),
            pltpu.VMEM((4, cap, quarter), bf16),
            pltpu.VMEM((4, cap, quarter), bf16),
            dma((2 * hid_tiles + 9,)),
            dma((6,)),
            dma((4, 2)),
            dma((4, 2)),
            dma((3, 4, 2)),
            dma((3, 4, 2)),
            dma((2, 4)),
            dma((2, 4)),
            dma((4, 2)),
            dma((4, 2)),
            dma((4, 2)),
            dma((4, 2)),
            dma((2, 3)),
            dma((2, 3)),
            dma((2,)),
        ],
        compiler_params=pltpu.CompilerParams(
            collective_id=0, has_side_effects=True, vmem_limit_bytes=56 << 20
        ),
    )(
        exp_input,
        norm_gain.reshape(1, -1),
        routes.T,
        route_weights.T,
        mix_input,
        pool_gain.reshape(1, -1),
        group_weight,
        branch_weight,
        gate_weight,
        up_weight,
        down_weight,
    )
    return pl.pallas_call(
        store_kernel,
        out_shape=(
            jax.ShapeDtypeStruct((rows_mix, quarter), bf16),
            jax.ShapeDtypeStruct((tokens, quarter), bf16),
        ),
        in_specs=[vmem] * 2,
        out_specs=(anywhere, anywhere),
        scratch_shapes=[dma((2,))],
    )(
        pltpu.with_memory_space_constraint(mix_out, pltpu.VMEM),
        pltpu.with_memory_space_constraint(exp_out, pltpu.VMEM),
    )


def fits(mesh, args):
    mix, group, _, _, tok, _, routes, _, gate, _, _ = args
    ep, tp, grp = (mesh.shape[k] for k in ("ep", "tp", "grp"))
    if ep != 4 or tp != 4 or routes.shape[1] != 2 or gate.shape[0] != ep:
        return False
    rows, channels = mix.shape[0] // (grp * ep), mix.shape[1] // tp
    tokens, quarter = tok.shape[0] // (grp * ep), tok.shape[1] // tp
    return (
        group.shape[1] == lanes
        and channels % (4 * lanes) == 0
        and channels == quarter
        and rows % 32 == 0
        and tokens % 64 == 0
        and gate.shape[2] % (tp * lanes) == 0
        and gate.shape[1] * gate.shape[2] <= 1 << 23
        and rows <= 512
        and tokens <= 256
    )


def solution(mesh):
    def run(*args):
        body = fused if fits(mesh, args) else on_device
        return jax.shard_map(
            body,
            mesh=mesh,
            in_specs=(
                P(("grp", "ep"), "tp"),
                P(),
                P(),
                P("tp", None),
                P(("grp", "ep"), None),
                P(),
                P(("grp", "ep"), None),
                P(("grp", "ep"), None),
                P("ep", None, "tp"),
                P("ep", None, "tp"),
                P("ep", "tp", None),
            ),
            out_specs=(P(("grp", "ep"), "tp"), P(("grp", "ep"), "tp")),
            check_vma=False,
        )(*args)

    return run
```

```python
import functools

import jax
import jax.numpy as jnp
from jax import lax
from jax.experimental import pallas as pl
from jax.experimental.pallas import tpu as pltpu
from jax.sharding import PartitionSpec as P

windows = (2, 4, 8, 16)
epsilon = 1e-06


def shifted(block, axis, distance):
    devices = range(lax.axis_size(axis))
    route = [(i - distance, i) for i in devices if i - distance in devices]
    return lax.ppermute(block, axis, route)


def trailing_sums(extended, rows):
    span_two = extended[1:] + extended[:-1]
    span_four = span_two[2:] + span_two[:-2]
    span_eight = span_four[4:] + span_four[:-4]
    span_sixteen = span_eight[8:] + span_eight[:-8]
    return [span_two[-rows:], span_four[-rows:], span_eight[-rows:], span_sixteen]


def pooled_deviation(extended, positions, group_ids, group_width, rows):
    sums = trailing_sums(extended, rows)
    current = extended[-rows:]
    window_id = jnp.repeat(group_ids % 4, group_width)
    result = jnp.zeros_like(current)
    for window_level, window_len in enumerate(windows):
        counted = jnp.minimum(positions + 1, window_len).astype(jnp.float32)[:, None]
        result = jnp.where(
            window_id[None, :] == window_level, sums[window_level] / counted - current, result
        )
    return result


def on_device(
    mix_input,
    group_weight,
    pool_gain,
    branch_weight,
    exp_input,
    norm_gain,
    routes,
    route_weights,
    gate_weight,
    up_weight,
    down_weight,
):
    tp_rank = lax.axis_index("tp")
    ep_rank = lax.axis_index("ep")
    rows_mix, channels = mix_input.shape
    group_width = group_weight.shape[1]
    group_count = channels // group_width
    first_group = tp_rank * group_count
    last_rows = mix_input[rows_mix - 15 :]
    before = shifted(last_rows, "ep", 1)
    extended = jnp.concatenate([before, mix_input], axis=0).astype(jnp.float32)
    positions = ep_rank * rows_mix + jnp.arange(rows_mix, dtype=jnp.int32)
    group_ids = first_group + jnp.arange(group_count, dtype=jnp.int32)
    deviation = pooled_deviation(extended, positions, group_ids, group_width, rows_mix).astype(
        jnp.bfloat16
    )
    own_groups = lax.dynamic_slice_in_dim(group_weight, first_group, group_count, 0)
    grouped = jnp.einsum(
        "rgc,gcd->rgd",
        deviation.reshape(rows_mix, group_count, group_width),
        own_groups,
        preferred_element_type=jnp.float32,
    ).reshape(rows_mix, channels)
    own_gain = lax.dynamic_slice_in_dim(pool_gain, first_group * group_width, channels, 0)
    pooled = (grouped * own_gain).astype(jnp.bfloat16)
    tok_rows, width = exp_input.shape
    columns = width // lax.axis_size("tp")
    experts_all = lax.axis_size("ep")
    capacity = 3 * tok_rows // experts_all
    floated = exp_input.astype(jnp.float32)
    normed = (
        floated
        * lax.rsqrt(jnp.mean(floated * floated, axis=1, keepdims=True) + epsilon)
        * norm_gain
    ).astype(jnp.bfloat16)
    flat_expert = routes.reshape(-1)
    assignments = flat_expert.shape[0]
    onehot = (flat_expert[:, None] == jnp.arange(experts_all, dtype=jnp.int32)[None, :]).astype(
        jnp.int32
    )
    slot_rank = jnp.sum((jnp.cumsum(onehot, axis=0) - onehot) * onehot, axis=1)
    slot_index = flat_expert * capacity + slot_rank
    token_of = jnp.arange(assignments, dtype=jnp.int32) // routes.shape[1]
    slot_token = (
        jnp.full((experts_all * capacity,), tok_rows, jnp.int32).at[slot_index].set(token_of)
    )
    padded = jnp.concatenate([normed, jnp.zeros((1, width), jnp.bfloat16)], axis=0)
    w_gate = gate_weight[0]
    w_up = up_weight[0]
    w_down = down_weight[0]
    arrived_rows = experts_all * capacity
    own_columns = lax.dynamic_slice_in_dim(padded, tp_rank * columns, columns, 1)
    outgoing = own_columns[slot_token].reshape(experts_all, capacity, columns)
    arrived = lax.all_to_all(outgoing, "ep", split_axis=0, concat_axis=0, tiled=True).reshape(
        arrived_rows, columns
    )
    section = lax.all_gather(arrived, "tp", axis=1, tiled=True)
    gate_pre = jnp.dot(section, w_gate, preferred_element_type=jnp.float32)
    up_pre = jnp.dot(section, w_up, preferred_element_type=jnp.float32)
    hidden = (jax.nn.silu(gate_pre) * up_pre).astype(jnp.bfloat16)
    weight_cols = branch_weight
    mix_sum = lax.psum_scatter(
        lax.dot_general(
            weight_cols, pooled, (((0,), (1,)), ((), ())), preferred_element_type=jnp.float32
        ).astype(jnp.bfloat16),
        "tp",
        scatter_dimension=0,
        tiled=True,
    )
    weight_cols = w_down
    exp_sum = lax.psum_scatter(
        lax.dot_general(
            weight_cols, hidden, (((0,), (1,)), ((), ())), preferred_element_type=jnp.float32
        ).astype(jnp.bfloat16),
        "tp",
        scatter_dimension=0,
        tiled=True,
    )
    mix_out = mix_sum.T
    results = exp_sum.reshape(columns, experts_all, capacity)
    returned = lax.all_to_all(results, "ep", split_axis=1, concat_axis=1, tiled=True).reshape(
        columns, experts_all * capacity
    )
    picked = returned[:, slot_index].astype(jnp.float32)
    weighted = picked * route_weights.reshape(-1)[None, :]
    combined = jnp.sum(weighted.reshape(columns, tok_rows, routes.shape[1]), axis=2)
    exp_out = combined.T.astype(jnp.bfloat16)
    return (mix_out, exp_out)


lanes = 128
pieces = 2
MESH = pl.DeviceIdType.MESH
f32 = jnp.float32
bf16 = jnp.bfloat16


def fused_kernel(
    x_hbm,
    norm_hbm,
    routes_hbm,
    weights_hbm,
    mix_hbm,
    gain_hbm,
    groups_hbm,
    branch_hbm,
    gate_hbm,
    up_hbm,
    down_hbm,
    mix_out,
    exp_out,
    x_ref,
    norm_ref,
    routes_ref,
    weights_ref,
    mix_ref,
    gain_ref,
    wgu,
    wd,
    wb,
    gw,
    xn,
    sb,
    xg,
    gu,
    hid,
    halo,
    pooled,
    keep_m,
    ps_m,
    pr_m,
    xs_m,
    xr_m,
    keep,
    ps,
    pr,
    xs,
    xr,
    zs,
    zr,
    w_sem,
    i_sem,
    s_sem,
    d_recv,
    f_recv,
    g_recv,
    p_recv,
    r_recv,
    z_recv,
    m_recv,
    h_sem,
):
    z = lax.axis_index("ep")
    t = lax.axis_index("tp")
    near = t + 1 - 2 * (t % 2)
    across = (t + 2) % 4
    diagonal = (near + 2) % 4
    inner = ((z + 1) // 2) % 2
    peers = [z, z + 1 - 2 * (z % 2), 3 - z, (z + 2) % 4]
    landing = 3 - inner
    slots = [0, 3, 2 - inner, 1 + inner]
    homes = [0, 2 + inner, 3 - 2 * inner, 1 + inner]
    home_of = [
        z,
        inner * peers[3] + (1 - inner) * peers[2],
        inner * peers[1] + (1 - inner) * peers[3],
        inner * peers[2] + (1 - inner) * peers[1],
    ]
    second = inner * across + (1 - inner) * near
    third = inner * near + (1 - inner) * across
    early = [None, (t, near), (t, second), (t, third)]
    late = [None, (across, diagonal), (third, diagonal), (second, diagonal)]
    tokens, width = x_ref.shape
    quarter = width // 4
    cap = xg.shape[2]
    piece = cap // pieces
    hid_tiles = gate_hbm.shape[2] // lanes
    rows_mix, channels = mix_ref.shape
    half_mix = rows_mix // 2
    group_count = channels // lanes

    barrier = pltpu.get_barrier_semaphore()
    for k in (1, 2, 3):
        pl.semaphore_signal(barrier, inc=1, device_id={"ep": peers[k]}, device_id_type=MESH)
    for k in (near, across):
        pl.semaphore_signal(barrier, inc=1, device_id={"tp": k}, device_id_type=MESH)

    pairs = (
        (routes_hbm, routes_ref),
        (weights_hbm, weights_ref),
        (x_hbm, x_ref),
        (norm_hbm, norm_ref),
        (mix_hbm, mix_ref),
        (gain_hbm, gain_ref),
    )
    load_i = [pltpu.make_async_copy(src, dst, i_sem.at[i]) for i, (src, dst) in enumerate(pairs)]
    front = (hid_tiles + 1) // 2
    loads = []
    for i in range(2 * hid_tiles):
        src = gate_hbm if i < hid_tiles else up_hbm
        at = (i % hid_tiles) * lanes
        loads.append(
            pltpu.make_async_copy(
                src.at[0, :, pl.ds(at, lanes)],
                wgu.at[i // 2, :, pl.ds((i % 2) * lanes, lanes)],
                w_sem.at[0 if i // 2 < front else 1],
            )
        )
    load_b = [
        pltpu.make_async_copy(branch_hbm.at[:, pl.ds(k * quarter, quarter)], wb.at[k], w_sem.at[2])
        for k in range(4)
    ]
    load_d = [
        pltpu.make_async_copy(down_hbm.at[0, :, pl.ds(k * quarter, quarter)], wd.at[k], w_sem.at[3])
        for k in range(4)
    ]
    load_g = pltpu.make_async_copy(groups_hbm.at[pl.ds(t * group_count, group_count)], gw, w_sem.at[4])

    def loaded(ref, i):
        pltpu.make_async_copy(ref, ref, w_sem.at[i]).wait()

    for c in load_i:
        c.start()

    def remote(src, dst, send, recv, who):
        return pltpu.make_async_remote_copy(
            src_ref=src, dst_ref=dst, send_sem=send, recv_sem=recv, device_id=who, device_id_type=MESH
        )

    for c in load_i[:2]:
        c.wait()
    lane = lax.broadcasted_iota(jnp.int32, (tokens, lanes), 1)
    square = (tokens, tokens)
    diagonal_mask = lax.broadcasted_iota(jnp.int32, square, 0) == lax.broadcasted_iota(jnp.int32, square, 1)

    def column(row):
        spread = jnp.broadcast_to(row, square)
        return jnp.sum(jnp.where(diagonal_mask, spread, jnp.zeros_like(spread)), axis=1, keepdims=True)

    r0 = column(routes_ref[0:1, :].astype(f32)).astype(jnp.int32)
    r1 = column(routes_ref[1:2, :].astype(f32)).astype(jnp.int32)
    w0 = column(weights_ref[0:1, :])
    w1 = column(weights_ref[1:2, :])
    member = ((r0 == lane) | (r1 == lane)).astype(f32)
    above = (
        lax.broadcasted_iota(jnp.int32, (tokens, tokens), 0)
        > lax.broadcasted_iota(jnp.int32, (tokens, tokens), 1)
    ).astype(f32)
    rank = jnp.dot(above.astype(bf16), member.astype(bf16), preferred_element_type=f32)
    slot_lane = lax.broadcasted_iota(jnp.int32, (tokens, cap), 1)
    places = []
    shares = []
    for k in range(4):
        own = jnp.sum(jnp.where(lane == peers[k], rank, 0.0), axis=1, keepdims=True).astype(jnp.int32)
        named = (r0 == peers[k]) | (r1 == peers[k])
        slot = jnp.where(named, own, cap)
        places.append((slot_lane == slot).astype(f32).astype(bf16))
        shares.append(
            jnp.where(r0 == peers[k], w0, 0.0)
            + jnp.where(r1 == peers[k], w1, 0.0)
        )

    for c in load_i[2:4]:
        c.wait()
    for c in [load_g] + load_b + loads + load_d:
        c.start()
    floated = x_ref[...].astype(f32)
    scale = lax.rsqrt(jnp.mean(floated * floated, axis=1, keepdims=True) + epsilon)
    xn_val = (floated * scale * norm_ref[...]).astype(bf16)
    for k in range(4):
        xn[k] = xn_val[:, k * quarter : (k + 1) * quarter]

    def gathered(k, block):
        return lax.dot_general(
            places[k], block, (((0,), (0,)), ((), ())), preferred_element_type=f32
        ).astype(bf16)

    def if_inner(step, k):
        pl.when(inner == 1)(lambda: step(k))

    def if_outer(step, k):
        pl.when(inner == 0)(lambda: step(k))

    own_cols = xn[t]
    for k in (2, 3):
        sb[k] = gathered(k, own_cols)
    for c in load_i[4:]:
        c.wait()
    pl.semaphore_wait(barrier, 5)

    def d_z(j, p):
        rows = pl.ds(p * piece, piece)
        q = across if j == 1 else t
        slot = 1 if j < 2 else landing
        at = j if j < 2 else landing
        return remote(
            sb.at[j, rows],
            xg.at[q, slot, rows],
            s_sem.at[0],
            d_recv.at[at, p],
            {"ep": peers[max(j, 1)]},
        )

    halo_copy = remote(
        mix_ref.at[pl.ds(rows_mix - 16, 16), :], halo, h_sem.at[0], h_sem.at[1], {"ep": (z + 1) % 4}
    )

    @pl.when(z < 3)
    def _():
        halo_copy.start()

    def send_rows(order):
        for j in order:
            for p in range(pieces):
                d_z(j, p).start()

    if_outer(send_rows, (2, 3))
    if_inner(send_rows, (3, 2))
    sb[0] = gathered(1, own_cols)
    sb[1] = gathered(1, xn[across])
    send_rows((0, 1))
    for q in range(4):
        xg[q, 0] = gathered(0, xn[q])

    def arrival(at, q, slot, p):
        rows = pl.ds(p * piece, piece)
        return remote(
            sb.at[0, rows], xg.at[q, slot, rows], s_sem.at[0], d_recv.at[at, p], {"ep": peers[1]}
        )

    def forward(i, q, slot, p):
        rows = pl.ds(p * piece, piece)
        block = xg.at[q, slot, rows]
        landed = f_recv.at[slot, p] if i == 0 else g_recv.at[i - 1, slot]
        return remote(block, block, s_sem.at[1], landed, {"tp": across if i == 0 else near})

    def from_z(k):
        if k == 1:
            for p in range(pieces):
                arrival(0, t, 1, p).wait_recv()
                forward(1, t, 1, p).start()
            for p in range(pieces):
                arrival(1, across, 1, p).wait_recv()
                forward(2, across, 1, p).start()
            return
        for p in range(pieces):
            arrival(k, t, k, p).wait_recv()
            forward(0, t, k, p).start()
            forward(1, t, k, p).start()

    def from_x(k):
        for p in range(pieces):
            forward(0, across, k, p).wait_recv()
            forward(2, across, k, p).start()

    def near_own(k):
        block = xg.at[near, k]
        remote(block, block, s_sem.at[1], g_recv.at[0, k], {"tp": near}).wait_recv()

    def near_other(k):
        block = xg.at[diagonal, k]
        remote(block, block, s_sem.at[1], g_recv.at[1, k], {"tp": near}).wait_recv()

    def mix_half(h):
        rows = slice(h * half_mix, (h + 1) * half_mix)
        position = z * rows_mix + h * half_mix + lax.broadcasted_iota(jnp.int32, (half_mix, lanes), 0)
        for g in range(group_count):
            cols = slice(g * lanes, (g + 1) * lanes)
            current = mix_ref[rows, cols].astype(f32)
            if h == 0:
                past = halo[:, cols].astype(f32)
            else:
                past = mix_ref[h * half_mix - 16 : h * half_mix, cols].astype(f32)
            total = jnp.concatenate([past, current], axis=0)
            level = g % 4
            for step in range(level + 1):
                total = total + pltpu.roll(total, 1 << step, 0)
            counted = jnp.minimum(position + 1, windows[level]).astype(f32)
            deviation = (total[16:] / counted - current).astype(bf16)
            grouped = jnp.dot(deviation, gw[g], preferred_element_type=f32)
            gain = gain_ref[:, pl.ds(pl.multiple_of(t * channels + g * lanes, lanes), lanes)]
            pooled[rows, cols] = (grouped * gain).astype(bf16)
        for i, q in enumerate((diagonal, near)):
            ps_m[h, i] = jnp.dot(pooled[rows], wb[q], preferred_element_type=f32).astype(bf16)
        for i, q in enumerate((across, t)):
            keep_m[h, i] = jnp.dot(pooled[rows], wb[q], preferred_element_type=f32)
        for i in range(2):
            m_p(h, i).start()

    def m_p(h, i):
        return remote(ps_m.at[h, i], pr_m.at[h, i], s_sem.at[5], m_recv.at[h, i], {"tp": near})

    def m_x(h):
        return remote(xs_m.at[h], xr_m.at[h], s_sem.at[6], m_recv.at[h, 2], {"tp": across})

    def send_mix(h):
        m_p(h, 0).wait_recv()
        xs_m[h] = (keep_m[h, 0] + pr_m[h, 0].astype(f32)).astype(bf16)
        m_x(h).start()

    def finish_mix(h):
        m_p(h, 1).wait_recv()
        m_x(h).wait_recv()
        total = keep_m[h, 1] + pr_m[h, 1].astype(f32) + xr_m[h].astype(f32)
        mix_out[h * half_mix : (h + 1) * half_mix] = total.astype(bf16)

    def expand(k, blocks, first, last):
        for n in range(first, last):
            if k == 0 and n == 0:
                loaded(wgu.at[pl.ds(0, front)], 0)
            if k == 0 and n == front:
                loaded(wgu.at[pl.ds(front, hid_tiles - front)], 1)
            total = None if blocks is None or blocks is early[k] else gu[k, n]
            for q in range(4) if blocks is None else blocks:
                rows = pl.ds(q * quarter if blocks is None else pl.multiple_of(q * quarter, quarter), quarter)
                part = jnp.dot(xg[q, slots[k]], wgu[n, rows, :], preferred_element_type=f32)
                total = part if total is None else total + part
            gu[k, n] = total

    def expand_early(k):
        expand(k, early[k], 0, hid_tiles)

    def activate(k):
        for i in range(hid_tiles):
            m = hid_tiles + i
            gate = gu[k, i // 2, :, (i % 2) * lanes : (i % 2 + 1) * lanes]
            up = gu[k, m // 2, :, (m % 2) * lanes : (m % 2 + 1) * lanes]
            hid[k, :, i * lanes : (i + 1) * lanes] = (gate / (1.0 + jnp.exp(-gate)) * up).astype(bf16)

    def r_p(i, k):
        return remote(ps.at[i, k], pr.at[i, k], s_sem.at[2], p_recv.at[i, k], {"tp": near})

    def r_x(k, p):
        rows = pl.ds(p * piece, piece)
        return remote(xs.at[k, rows], xr.at[k, rows], s_sem.at[3], r_recv.at[k, p], {"tp": across})

    def r_z(k, p):
        rows = pl.ds(p * piece, piece)
        return remote(
            zs.at[k, rows],
            zr.at[homes[k], rows],
            s_sem.at[4],
            z_recv.at[homes[k]],
            {"ep": home_of[k]},
        )

    def project(k):
        for i, q in enumerate((diagonal, near, across, t)):
            part = jnp.dot(hid[k], wd[q], preferred_element_type=f32)
            if i < 2:
                ps[i, k] = part.astype(bf16)
            else:
                keep[i - 2, k] = part
            if i == 0:
                r_p(0, k).start()
        r_p(1, k).start()

    def send_x(k):
        r_p(0, k).wait_recv()
        for p in range(pieces):
            rows = slice(p * piece, (p + 1) * piece)
            xs[k, rows] = (keep[0, k, rows] + pr[0, k, rows].astype(f32)).astype(bf16)
            r_x(k, p).start()

    def send_z(k, first=0, last=pieces):
        if first == 0:
            r_p(1, k).wait_recv()
        for p in range(first, last):
            rows = slice(p * piece, (p + 1) * piece)
            r_x(k, p).wait_recv()
            zs[k, rows] = (keep[1, k, rows] + pr[1, k, rows].astype(f32) + xr[k, rows].astype(f32)).astype(bf16)
            if k > 0:
                r_z(k, p).start()

    def share(k):
        block = zs[0] if k == 0 else zr[k]
        return shares[k] * jnp.dot(places[k], block, preferred_element_type=f32)

    def returned(k):
        remote(zs.at[k], zr.at[k], s_sem.at[4], z_recv.at[k], {"ep": peers[k]}).wait_recv()

    def left(ref, i):
        remote(ref, ref, s_sem.at[i], s_sem.at[i], {"tp": near}).wait_send()

    half = hid_tiles // 2
    load_g.wait()
    loaded(wb, 2)
    mix_half(1)
    expand(0, None, 0, half)
    send_mix(1)
    expand(0, None, half, hid_tiles)
    activate(0)
    loaded(wd, 3)
    project(0)
    if_outer(from_z, 3)

    @pl.when(z == 0)
    def _():
        halo[...] = jnp.zeros_like(halo)

    @pl.when(z > 0)
    def _():
        halo_copy.wait_recv()

    mix_half(0)
    if_inner(from_z, 3)
    near_own(3)
    expand(1, early[1], 0, hid_tiles)
    if_outer(from_z, 2)
    if_outer(from_x, 3)
    from_z(1)
    if_inner(from_z, 2)
    if_inner(from_x, 3)
    expand(1, late[1][:1], 0, hid_tiles)
    if_outer(near_own, 2)
    expand(2, early[2], 0, hid_tiles)
    send_x(0)
    near_other(3)
    expand(1, late[1][1:], 0, hid_tiles)
    activate(1)
    project(1)
    if_outer(from_x, 2)
    if_outer(send_x, 1)
    if_outer(send_mix, 0)
    if_outer(expand_early, 3)
    if_inner(near_own, 1)
    if_inner(near_other, 1)
    if_outer(near_other, 2)
    expand(2, late[2], 0, half)
    if_inner(send_x, 1)
    expand(2, late[2], half, hid_tiles)
    activate(2)
    if_inner(from_x, 2)
    project(2)
    if_inner(near_own, 2)
    if_inner(expand_early, 3)
    if_outer(near_own, 1)
    if_outer(near_other, 1)
    if_inner(send_x, 2)
    if_inner(near_other, 2)
    expand(3, late[3], 0, half)
    if_outer(send_x, 2)
    expand(3, late[3], half, hid_tiles)
    activate(3)
    if_outer(send_z, 1)
    project(3)
    if_inner(send_z, 1)
    send_x(3)
    if_inner(send_mix, 0)
    send_z(2)
    send_z(3)
    send_z(0)
    finish_mix(1)
    result = share(0)
    left(sb, 0)
    left(xg.at[pl.ds(0, 2)], 1)
    left(ps, 2)
    left(xs, 3)
    left(ps_m, 5)

    @pl.when(z < 3)
    def _():
        halo_copy.wait_send()

    returned(3)
    result = result + share(3)
    finish_mix(0)
    for k in (1, 2):
        returned(k)
        result = result + share(k)
    exp_out[...] = result.astype(bf16)

    left(xs_m, 6)
    left(zs.at[pl.ds(1, 3)], 4)


def store_kernel(mix_ref, exp_ref, mix_hbm, exp_hbm, sem):
    stores = [
        pltpu.make_async_copy(mix_ref, mix_hbm, sem.at[0]),
        pltpu.make_async_copy(exp_ref, exp_hbm, sem.at[1]),
    ]
    for c in stores:
        c.start()
    for c in stores:
        c.wait()


def fused(
    mix_input,
    group_weight,
    pool_gain,
    branch_weight,
    exp_input,
    norm_gain,
    routes,
    route_weights,
    gate_weight,
    up_weight,
    down_weight,
):
    tokens, width = exp_input.shape
    rows_mix, channels = mix_input.shape
    hidden = gate_weight.shape[2]
    quarter = width // 4
    cap = 3 * tokens // 4
    hid_tiles = hidden // lanes
    half_mix = rows_mix // 2
    vmem = pl.BlockSpec(memory_space=pltpu.VMEM)
    anywhere = pl.BlockSpec(memory_space=pl.ANY)
    dma = pltpu.SemaphoreType.DMA
    mix_out, exp_out = pl.pallas_call(
        fused_kernel,
        out_shape=(
            pltpu.VMEM((rows_mix, quarter), bf16),
            pltpu.VMEM((tokens, quarter), bf16),
        ),
        in_specs=[anywhere] * 11,
        out_specs=(vmem, vmem),
        scratch_shapes=[
            pltpu.VMEM((tokens, width), bf16),
            pltpu.VMEM((1, width), f32),
            pltpu.VMEM((2, tokens), jnp.int32),
            pltpu.VMEM((2, tokens), f32),
            pltpu.VMEM((rows_mix, channels), bf16),
            pltpu.VMEM((1, 4 * channels), f32),
            pltpu.VMEM((hid_tiles, width, 2 * lanes), bf16),
            pltpu.VMEM((4, hidden, quarter), bf16),
            pltpu.VMEM((4, channels, quarter), bf16),
            pltpu.VMEM((channels // lanes, lanes, lanes), bf16),
            pltpu.VMEM((4, tokens, quarter), bf16),
            pltpu.VMEM((4, cap, quarter), bf16),
            pltpu.VMEM((4, 4, cap, quarter), bf16),
            pltpu.VMEM((4, hid_tiles, cap, 2 * lanes), f32),
            pltpu.VMEM((4, cap, hidden), bf16),
            pltpu.VMEM((16, channels), bf16),
            pltpu.VMEM((rows_mix, channels), bf16),
            pltpu.VMEM((2, 2, half_mix, quarter), f32),
            pltpu.VMEM((2, 2, half_mix, quarter), bf16),
            pltpu.VMEM((2, 2, half_mix, quarter), bf16),
            pltpu.VMEM((2, half_mix, quarter), bf16),
            pltpu.VMEM((2, half_mix, quarter), bf16),
            pltpu.VMEM((2, 4, cap, quarter), f32),
            pltpu.VMEM((2, 4, cap, quarter), bf16),
            pltpu.VMEM((2, 4, cap, quarter), bf16),
            pltpu.VMEM((4, cap, quarter), bf16),
            pltpu.VMEM((4, cap, quarter), bf16),
            pltpu.VMEM((4, cap, quarter), bf16),
            pltpu.VMEM((4, cap, quarter), bf16),
            dma((5,)),
            dma((6,)),
            dma((7,)),
            dma((4, pieces)),
            dma((4, pieces)),
            dma((2, 4)),
            dma((2, 4)),
            dma((4, pieces)),
            dma((4,)),
            dma((2, 3)),
            dma((2,)),
        ],
        compiler_params=pltpu.CompilerParams(
            collective_id=0, has_side_effects=True, vmem_limit_bytes=56 << 20
        ),
    )(
        exp_input,
        norm_gain.reshape(1, -1),
        routes.T,
        route_weights.T,
        mix_input,
        pool_gain.reshape(1, -1),
        group_weight,
        branch_weight,
        gate_weight,
        up_weight,
        down_weight,
    )
    return pl.pallas_call(
        store_kernel,
        out_shape=(
            jax.ShapeDtypeStruct((rows_mix, quarter), bf16),
            jax.ShapeDtypeStruct((tokens, quarter), bf16),
        ),
        in_specs=[vmem] * 2,
        out_specs=(anywhere, anywhere),
        scratch_shapes=[dma((2,))],
    )(
        pltpu.with_memory_space_constraint(mix_out, pltpu.VMEM),
        pltpu.with_memory_space_constraint(exp_out, pltpu.VMEM),
    )


def fits(mesh, args):
    mix, group, _, _, tok, _, routes, _, gate, _, _ = args
    ep, tp, grp = (mesh.shape[k] for k in ("ep", "tp", "grp"))
    if ep != 4 or tp != 4 or routes.shape[1] != 2 or gate.shape[0] != ep:
        return False
    rows, channels = mix.shape[0] // (grp * ep), mix.shape[1] // tp
    tokens, quarter = tok.shape[0] // (grp * ep), tok.shape[1] // tp
    return (
        group.shape[1] == lanes
        and channels % (4 * lanes) == 0
        and channels == quarter
        and rows % 32 == 0
        and tokens % 64 == 0
        and gate.shape[2] % (tp * lanes) == 0
        and gate.shape[1] * gate.shape[2] <= 1 << 23
        and rows <= 512
        and tokens <= 256
    )


def solution(mesh):
    def run(*args):
        body = fused if fits(mesh, args) else on_device
        return jax.shard_map(
            body,
            mesh=mesh,
            in_specs=(
                P(("grp", "ep"), "tp"),
                P(),
                P(),
                P("tp", None),
                P(("grp", "ep"), None),
                P(),
                P(("grp", "ep"), None),
                P(("grp", "ep"), None),
                P("ep", None, "tp"),
                P("ep", None, "tp"),
                P("ep", "tp", None),
            ),
            out_specs=(P(("grp", "ep"), "tp"), P(("grp", "ep"), "tp")),
            check_vma=False,
        )(*args)

    return run
```

```python
import functools

import jax
import jax.numpy as jnp
from jax import lax
from jax.experimental import pallas as pl
from jax.experimental.pallas import tpu as pltpu
from jax.sharding import PartitionSpec as P

windows = (2, 4, 8, 16)
epsilon = 1e-06


def shifted(block, axis, distance):
    devices = range(lax.axis_size(axis))
    route = [(i - distance, i) for i in devices if i - distance in devices]
    return lax.ppermute(block, axis, route)


def trailing_sums(extended, rows):
    span_two = extended[1:] + extended[:-1]
    span_four = span_two[2:] + span_two[:-2]
    span_eight = span_four[4:] + span_four[:-4]
    span_sixteen = span_eight[8:] + span_eight[:-8]
    return [span_two[-rows:], span_four[-rows:], span_eight[-rows:], span_sixteen]


def pooled_deviation(extended, positions, group_ids, group_width, rows):
    sums = trailing_sums(extended, rows)
    current = extended[-rows:]
    window_id = jnp.repeat(group_ids % 4, group_width)
    result = jnp.zeros_like(current)
    for window_level, window_len in enumerate(windows):
        counted = jnp.minimum(positions + 1, window_len).astype(jnp.float32)[:, None]
        result = jnp.where(
            window_id[None, :] == window_level, sums[window_level] / counted - current, result
        )
    return result


def on_device(
    mix_input,
    group_weight,
    pool_gain,
    branch_weight,
    exp_input,
    norm_gain,
    routes,
    route_weights,
    gate_weight,
    up_weight,
    down_weight,
):
    tp_rank = lax.axis_index("tp")
    ep_rank = lax.axis_index("ep")
    rows_mix, channels = mix_input.shape
    group_width = group_weight.shape[1]
    group_count = channels // group_width
    first_group = tp_rank * group_count
    last_rows = mix_input[rows_mix - 15 :]
    before = shifted(last_rows, "ep", 1)
    extended = jnp.concatenate([before, mix_input], axis=0).astype(jnp.float32)
    positions = ep_rank * rows_mix + jnp.arange(rows_mix, dtype=jnp.int32)
    group_ids = first_group + jnp.arange(group_count, dtype=jnp.int32)
    deviation = pooled_deviation(extended, positions, group_ids, group_width, rows_mix).astype(
        jnp.bfloat16
    )
    own_groups = lax.dynamic_slice_in_dim(group_weight, first_group, group_count, 0)
    grouped = jnp.einsum(
        "rgc,gcd->rgd",
        deviation.reshape(rows_mix, group_count, group_width),
        own_groups,
        preferred_element_type=jnp.float32,
    ).reshape(rows_mix, channels)
    own_gain = lax.dynamic_slice_in_dim(pool_gain, first_group * group_width, channels, 0)
    pooled = (grouped * own_gain).astype(jnp.bfloat16)
    tok_rows, width = exp_input.shape
    columns = width // lax.axis_size("tp")
    experts_all = lax.axis_size("ep")
    capacity = 3 * tok_rows // experts_all
    floated = exp_input.astype(jnp.float32)
    normed = (
        floated
        * lax.rsqrt(jnp.mean(floated * floated, axis=1, keepdims=True) + epsilon)
        * norm_gain
    ).astype(jnp.bfloat16)
    flat_expert = routes.reshape(-1)
    assignments = flat_expert.shape[0]
    onehot = (flat_expert[:, None] == jnp.arange(experts_all, dtype=jnp.int32)[None, :]).astype(
        jnp.int32
    )
    slot_rank = jnp.sum((jnp.cumsum(onehot, axis=0) - onehot) * onehot, axis=1)
    slot_index = flat_expert * capacity + slot_rank
    token_of = jnp.arange(assignments, dtype=jnp.int32) // routes.shape[1]
    slot_token = (
        jnp.full((experts_all * capacity,), tok_rows, jnp.int32).at[slot_index].set(token_of)
    )
    padded = jnp.concatenate([normed, jnp.zeros((1, width), jnp.bfloat16)], axis=0)
    w_gate = gate_weight[0]
    w_up = up_weight[0]
    w_down = down_weight[0]
    arrived_rows = experts_all * capacity
    own_columns = lax.dynamic_slice_in_dim(padded, tp_rank * columns, columns, 1)
    outgoing = own_columns[slot_token].reshape(experts_all, capacity, columns)
    arrived = lax.all_to_all(outgoing, "ep", split_axis=0, concat_axis=0, tiled=True).reshape(
        arrived_rows, columns
    )
    section = lax.all_gather(arrived, "tp", axis=1, tiled=True)
    gate_pre = jnp.dot(section, w_gate, preferred_element_type=jnp.float32)
    up_pre = jnp.dot(section, w_up, preferred_element_type=jnp.float32)
    hidden = (jax.nn.silu(gate_pre) * up_pre).astype(jnp.bfloat16)
    weight_cols = branch_weight
    mix_sum = lax.psum_scatter(
        lax.dot_general(
            weight_cols, pooled, (((0,), (1,)), ((), ())), preferred_element_type=jnp.float32
        ).astype(jnp.bfloat16),
        "tp",
        scatter_dimension=0,
        tiled=True,
    )
    weight_cols = w_down
    exp_sum = lax.psum_scatter(
        lax.dot_general(
            weight_cols, hidden, (((0,), (1,)), ((), ())), preferred_element_type=jnp.float32
        ).astype(jnp.bfloat16),
        "tp",
        scatter_dimension=0,
        tiled=True,
    )
    mix_out = mix_sum.T
    results = exp_sum.reshape(columns, experts_all, capacity)
    returned = lax.all_to_all(results, "ep", split_axis=1, concat_axis=1, tiled=True).reshape(
        columns, experts_all * capacity
    )
    picked = returned[:, slot_index].astype(jnp.float32)
    weighted = picked * route_weights.reshape(-1)[None, :]
    combined = jnp.sum(weighted.reshape(columns, tok_rows, routes.shape[1]), axis=2)
    exp_out = combined.T.astype(jnp.bfloat16)
    return (mix_out, exp_out)


lanes = 128
pieces = 2
MESH = pl.DeviceIdType.MESH
f32 = jnp.float32
bf16 = jnp.bfloat16


def fused_kernel(
    x_hbm,
    norm_hbm,
    routes_hbm,
    weights_hbm,
    mix_hbm,
    gain_hbm,
    groups_hbm,
    branch_hbm,
    gate_hbm,
    up_hbm,
    down_hbm,
    mix_out,
    exp_out,
    x_ref,
    norm_ref,
    routes_ref,
    weights_ref,
    mix_ref,
    gain_ref,
    wgu,
    wd,
    wb,
    gw,
    xn,
    sb,
    xg,
    gu,
    hid,
    halo,
    pooled,
    keep_m,
    ps_m,
    pr_m,
    xs_m,
    xr_m,
    keep,
    ps,
    pr,
    xs,
    xr,
    zs,
    zr,
    w_sem,
    i_sem,
    s_sem,
    d_recv,
    f_recv,
    g_recv,
    p_recv,
    r_recv,
    z_recv,
    m_recv,
    h_sem,
):
    z = lax.axis_index("ep")
    t = lax.axis_index("tp")
    near = t + 1 - 2 * (t % 2)
    across = (t + 2) % 4
    diagonal = (near + 2) % 4
    inner = ((z + 1) // 2) % 2
    peers = [z, z + 1 - 2 * (z % 2), 3 - z, (z + 2) % 4]
    landing = 3 - inner
    slots = [0, 3, 2 - inner, 1 + inner]
    homes = [0, 2 + inner, 3 - 2 * inner, 1 + inner]
    home_of = [
        z,
        inner * peers[3] + (1 - inner) * peers[2],
        inner * peers[1] + (1 - inner) * peers[3],
        inner * peers[2] + (1 - inner) * peers[1],
    ]
    second = inner * across + (1 - inner) * near
    third = inner * near + (1 - inner) * across
    early = [None, (t, near), (t, second), (t, third)]
    late = [None, (across, diagonal), (third, diagonal), (second, diagonal)]
    tokens, width = x_ref.shape
    quarter = width // 4
    cap = xg.shape[2]
    piece = cap // pieces
    hid_tiles = gate_hbm.shape[2] // lanes
    rows_mix, channels = mix_ref.shape
    half_mix = rows_mix // 2
    group_count = channels // lanes

    barrier = pltpu.get_barrier_semaphore()
    for k in (1, 2, 3):
        pl.semaphore_signal(barrier, inc=1, device_id={"ep": peers[k]}, device_id_type=MESH)
    for k in (near, across):
        pl.semaphore_signal(barrier, inc=1, device_id={"tp": k}, device_id_type=MESH)

    pairs = (
        (routes_hbm, routes_ref),
        (weights_hbm, weights_ref),
        (x_hbm, x_ref),
        (norm_hbm, norm_ref),
        (mix_hbm, mix_ref),
        (gain_hbm, gain_ref),
    )
    part = tokens // 4
    load_x = [
        pltpu.make_async_copy(x_hbm.at[pl.ds(i * part, part)], x_ref.at[pl.ds(i * part, part)], i_sem.at[2])
        for i in range(4)
    ]
    load_i = [pltpu.make_async_copy(src, dst, i_sem.at[i]) for i, (src, dst) in enumerate(pairs)]
    front = (hid_tiles + 1) // 2
    loads = []
    for i in range(2 * hid_tiles):
        src = gate_hbm if i < hid_tiles else up_hbm
        at = (i % hid_tiles) * lanes
        loads.append(
            pltpu.make_async_copy(
                src.at[0, :, pl.ds(at, lanes)],
                wgu.at[i // 2, :, pl.ds((i % 2) * lanes, lanes)],
                w_sem.at[0 if i // 2 < front else 1],
            )
        )
    load_b = [
        pltpu.make_async_copy(branch_hbm.at[:, pl.ds(k * quarter, quarter)], wb.at[k], w_sem.at[2])
        for k in range(4)
    ]
    load_d = [
        pltpu.make_async_copy(down_hbm.at[0, :, pl.ds(k * quarter, quarter)], wd.at[k], w_sem.at[3])
        for k in range(4)
    ]
    load_g = pltpu.make_async_copy(groups_hbm.at[pl.ds(t * group_count, group_count)], gw, w_sem.at[4])

    def loaded(ref, i):
        pltpu.make_async_copy(ref, ref, w_sem.at[i]).wait()

    for c in load_i[:2] + load_x + load_i[3:]:
        c.start()

    def remote(src, dst, send, recv, who):
        return pltpu.make_async_remote_copy(
            src_ref=src, dst_ref=dst, send_sem=send, recv_sem=recv, device_id=who, device_id_type=MESH
        )

    for c in load_i[:2]:
        c.wait()
    lane = lax.broadcasted_iota(jnp.int32, (tokens, lanes), 1)
    square = (tokens, tokens)
    diagonal_mask = lax.broadcasted_iota(jnp.int32, square, 0) == lax.broadcasted_iota(jnp.int32, square, 1)

    def column(row):
        spread = jnp.broadcast_to(row, square)
        return jnp.sum(jnp.where(diagonal_mask, spread, jnp.zeros_like(spread)), axis=1, keepdims=True)

    r0 = column(routes_ref[0:1, :].astype(f32)).astype(jnp.int32)
    r1 = column(routes_ref[1:2, :].astype(f32)).astype(jnp.int32)
    w0 = column(weights_ref[0:1, :])
    w1 = column(weights_ref[1:2, :])
    member = ((r0 == lane) | (r1 == lane)).astype(f32)
    above = (
        lax.broadcasted_iota(jnp.int32, (tokens, tokens), 0)
        > lax.broadcasted_iota(jnp.int32, (tokens, tokens), 1)
    ).astype(f32)
    rank = jnp.dot(above.astype(bf16), member.astype(bf16), preferred_element_type=f32)
    slot_lane = lax.broadcasted_iota(jnp.int32, (tokens, cap), 1)
    places = []
    shares = []
    for k in range(4):
        own = jnp.sum(jnp.where(lane == peers[k], rank, 0.0), axis=1, keepdims=True).astype(jnp.int32)
        named = (r0 == peers[k]) | (r1 == peers[k])
        slot = jnp.where(named, own, cap)
        places.append((slot_lane == slot).astype(f32).astype(bf16))
        shares.append(
            jnp.where(r0 == peers[k], w0, 0.0)
            + jnp.where(r1 == peers[k], w1, 0.0)
        )

    for c in load_i[2:4]:
        c.wait()
    for c in [load_g] + load_b + loads + load_d:
        c.start()
    floated = x_ref[...].astype(f32)
    scale = lax.rsqrt(jnp.mean(floated * floated, axis=1, keepdims=True) + epsilon)
    xn_val = (floated * scale * norm_ref[...]).astype(bf16)
    for k in range(4):
        xn[k] = xn_val[:, k * quarter : (k + 1) * quarter]

    def gathered(k, block):
        return lax.dot_general(
            places[k], block, (((0,), (0,)), ((), ())), preferred_element_type=f32
        ).astype(bf16)

    def if_inner(step, *k):
        pl.when(inner == 1)(lambda: step(*k))

    def if_outer(step, *k):
        pl.when(inner == 0)(lambda: step(*k))

    own_cols = xn[t]
    for k in (2, 3):
        sb[k] = gathered(k, own_cols)
    for c in load_i[4:]:
        c.wait()
    pl.semaphore_wait(barrier, 5)

    def d_z(j, p):
        rows = pl.ds(p * piece, piece)
        q = across if j == 1 else t
        slot = 1 if j < 2 else landing
        at = j if j < 2 else landing
        return remote(
            sb.at[j, rows],
            xg.at[q, slot, rows],
            s_sem.at[0],
            d_recv.at[at, p],
            {"ep": peers[max(j, 1)]},
        )

    halo_copy = remote(
        mix_ref.at[pl.ds(rows_mix - 16, 16), :], halo, h_sem.at[0], h_sem.at[1], {"ep": (z + 1) % 4}
    )

    @pl.when(z < 3)
    def _():
        halo_copy.start()

    def send_rows(order):
        for j in order:
            for p in range(pieces):
                d_z(j, p).start()

    if_outer(send_rows, (2, 3))
    if_inner(send_rows, (3, 2))
    sb[0] = gathered(1, own_cols)
    sb[1] = gathered(1, xn[across])
    send_rows((0, 1))
    for q in range(4):
        xg[q, 0] = gathered(0, xn[q])

    def arrival(at, q, slot, p):
        rows = pl.ds(p * piece, piece)
        return remote(
            sb.at[0, rows], xg.at[q, slot, rows], s_sem.at[0], d_recv.at[at, p], {"ep": peers[1]}
        )

    def forward(i, q, slot, p):
        rows = pl.ds(p * piece, piece)
        block = xg.at[q, slot, rows]
        landed = f_recv.at[slot - 2, p] if i == 0 else g_recv.at[i - 1, slot - 1]
        return remote(block, block, s_sem.at[1], landed, {"tp": across if i == 0 else near})

    def from_z(k):
        if k == 1:
            for p in range(pieces):
                arrival(0, t, 1, p).wait_recv()
                forward(1, t, 1, p).start()
            for p in range(pieces):
                arrival(1, across, 1, p).wait_recv()
                forward(2, across, 1, p).start()
            return
        for p in range(pieces):
            arrival(k, t, k, p).wait_recv()
            forward(0, t, k, p).start()
            forward(1, t, k, p).start()

    def from_x(k):
        for p in range(pieces):
            forward(0, across, k, p).wait_recv()
            forward(2, across, k, p).start()

    def near_own(k):
        block = xg.at[near, k]
        remote(block, block, s_sem.at[1], g_recv.at[0, k - 1], {"tp": near}).wait_recv()

    def near_other(k):
        block = xg.at[diagonal, k]
        remote(block, block, s_sem.at[1], g_recv.at[1, k - 1], {"tp": near}).wait_recv()

    def mix_half(h):
        rows = slice(h * half_mix, (h + 1) * half_mix)
        position = z * rows_mix + h * half_mix + lax.broadcasted_iota(jnp.int32, (half_mix, lanes), 0)
        for g in range(group_count):
            cols = slice(g * lanes, (g + 1) * lanes)
            current = mix_ref[rows, cols].astype(f32)
            if h == 0:
                past = halo[:, cols].astype(f32)
            else:
                past = mix_ref[h * half_mix - 16 : h * half_mix, cols].astype(f32)
            total = jnp.concatenate([past, current], axis=0)
            level = g % 4
            for step in range(level + 1):
                total = total + pltpu.roll(total, 1 << step, 0)
            counted = jnp.minimum(position + 1, windows[level]).astype(f32)
            deviation = (total[16:] / counted - current).astype(bf16)
            grouped = jnp.dot(deviation, gw[g], preferred_element_type=f32)
            gain = gain_ref[:, pl.ds(pl.multiple_of(t * channels + g * lanes, lanes), lanes)]
            pooled[rows, cols] = (grouped * gain).astype(bf16)
        for i, q in enumerate((diagonal, near)):
            ps_m[h, i] = jnp.dot(pooled[rows], wb[q], preferred_element_type=f32).astype(bf16)
        for i, q in enumerate((across, t)):
            keep_m[h, i] = jnp.dot(pooled[rows], wb[q], preferred_element_type=f32)
        for i in range(2):
            m_p(h, i).start()

    def m_p(h, i):
        return remote(ps_m.at[h, i], pr_m.at[h, i], s_sem.at[5], m_recv.at[h, i], {"tp": near})

    def m_x(h):
        return remote(xs_m.at[h], xr_m.at[h], s_sem.at[6], m_recv.at[h, 2], {"tp": across})

    def send_mix(h):
        m_p(h, 0).wait_recv()
        xs_m[h] = (keep_m[h, 0] + pr_m[h, 0].astype(f32)).astype(bf16)
        m_x(h).start()

    def finish_mix(h):
        m_p(h, 1).wait_recv()
        m_x(h).wait_recv()
        total = keep_m[h, 1] + pr_m[h, 1].astype(f32) + xr_m[h].astype(f32)
        mix_out[h * half_mix : (h + 1) * half_mix] = total.astype(bf16)

    def expand(k, blocks, first, last):
        for n in range(first, last):
            if k == 0 and n == 0:
                loaded(wgu.at[pl.ds(0, front)], 0)
            if k == 0 and n == front:
                loaded(wgu.at[pl.ds(front, hid_tiles - front)], 1)
            total = None if blocks is None or blocks is early[k] else gu[k, n]
            for q in range(4) if blocks is None else blocks:
                rows = pl.ds(q * quarter if blocks is None else pl.multiple_of(q * quarter, quarter), quarter)
                part = jnp.dot(xg[q, slots[k]], wgu[n, rows, :], preferred_element_type=f32)
                total = part if total is None else total + part
            gu[k, n] = total

    def expand_early(k, first, last):
        expand(k, early[k], first, last)

    def activate(k):
        for i in range(hid_tiles):
            m = hid_tiles + i
            gate = gu[k, i // 2, :, (i % 2) * lanes : (i % 2 + 1) * lanes]
            up = gu[k, m // 2, :, (m % 2) * lanes : (m % 2 + 1) * lanes]
            hid[k, :, i * lanes : (i + 1) * lanes] = (gate / (1.0 + jnp.exp(-gate)) * up).astype(bf16)

    def r_p(i, k):
        return remote(ps.at[i, k], pr.at[i, k], s_sem.at[2], p_recv.at[i, k], {"tp": near})

    def r_x(k, p):
        rows = pl.ds(p * piece, piece)
        return remote(xs.at[k, rows], xr.at[k, rows], s_sem.at[3], r_recv.at[k, p], {"tp": across})

    def r_z(k, p):
        rows = pl.ds(p * piece, piece)
        return remote(
            zs.at[k, rows],
            zr.at[homes[k], rows],
            s_sem.at[4],
            z_recv.at[homes[k] - 1],
            {"ep": home_of[k]},
        )

    def project(k, first=0, last=4):
        for i, q in list(enumerate((diagonal, near, across, t)))[first:last]:
            part = jnp.dot(hid[k], wd[q], preferred_element_type=f32)
            if i < 2:
                ps[i, k] = part.astype(bf16)
            else:
                keep[i - 2, k] = part
            if i == 0:
                r_p(0, k).start()
        if last == 4:
            r_p(1, k).start()

    def send_x(k):
        r_p(0, k).wait_recv()
        for p in range(pieces):
            rows = slice(p * piece, (p + 1) * piece)
            xs[k, rows] = (keep[0, k, rows] + pr[0, k, rows].astype(f32)).astype(bf16)
            r_x(k, p).start()

    def send_z(k, first=0, last=pieces):
        if first == 0:
            r_p(1, k).wait_recv()
        for p in range(first, last):
            rows = slice(p * piece, (p + 1) * piece)
            r_x(k, p).wait_recv()
            zs[k, rows] = (keep[1, k, rows] + pr[1, k, rows].astype(f32) + xr[k, rows].astype(f32)).astype(bf16)
            if k > 0:
                r_z(k, p).start()

    def share(k):
        block = zs[0] if k == 0 else zr[k]
        return shares[k] * jnp.dot(places[k], block, preferred_element_type=f32)

    def returned(k):
        remote(zs.at[k], zr.at[k], s_sem.at[4], z_recv.at[k - 1], {"ep": peers[k]}).wait_recv()

    def left(ref, i):
        remote(ref, ref, s_sem.at[i], s_sem.at[i], {"tp": near}).wait_send()

    half = hid_tiles // 2
    load_g.wait()
    loaded(wb, 2)
    mix_half(1)
    expand(0, None, 0, half)
    send_mix(1)
    expand(0, None, half, hid_tiles)
    activate(0)
    loaded(wd, 3)
    project(0)
    if_outer(from_z, 3)

    @pl.when(z == 0)
    def _():
        halo[...] = jnp.zeros_like(halo)

    @pl.when(z > 0)
    def _():
        halo_copy.wait_recv()

    mix_half(0)
    if_inner(from_z, 3)
    near_own(3)
    expand(1, early[1], 0, hid_tiles)
    if_outer(from_z, 2)
    if_outer(from_x, 3)
    if_inner(from_x, 3)
    from_z(1)
    if_inner(from_z, 2)
    expand(1, late[1][:1], 0, hid_tiles)
    if_outer(near_own, 2)
    if_outer(send_mix, 0)
    expand(2, early[2], 0, hid_tiles)
    if_inner(send_x, 0)
    near_other(3)
    expand(1, late[1][1:], 0, hid_tiles)
    activate(1)
    project(1)
    if_outer(from_x, 2)
    if_outer(send_x, 1)
    if_outer(send_x, 0)
    if_outer(expand_early, 3, 0, hid_tiles)
    if_inner(near_own, 1)
    if_inner(near_other, 1)
    if_outer(near_other, 2)
    expand(2, late[2], 0, half)
    if_inner(send_x, 1)
    expand(2, late[2], half, hid_tiles)
    activate(2)
    project(2, 0, 2)
    if_inner(from_x, 2)
    project(2, 2, 4)
    if_inner(near_own, 2)
    if_inner(expand_early, 3, 0, half)
    if_inner(send_x, 2)
    if_inner(expand_early, 3, half, hid_tiles)
    if_outer(near_own, 1)
    if_outer(near_other, 1)
    if_inner(near_other, 2)
    expand(3, late[3], 0, half)
    if_outer(send_x, 2)
    expand(3, late[3], half, hid_tiles)
    activate(3)
    if_outer(send_z, 1)
    if_inner(send_z, 1, 0, 1)
    project(3)
    if_inner(send_z, 1, 1, pieces)
    send_x(3)
    if_outer(send_z, 2, 0, 1)
    if_outer(send_z, 3, 0, 1)
    if_outer(send_z, 2, 1, pieces)
    if_outer(send_z, 3, 1, pieces)
    if_inner(send_z, 2)
    if_inner(send_mix, 0)
    if_inner(send_z, 3)
    send_z(0)
    finish_mix(1)
    result = share(0)
    left(sb, 0)
    left(xg.at[pl.ds(0, 2)], 1)
    left(ps, 2)
    left(xs, 3)
    left(ps_m, 5)

    @pl.when(z < 3)
    def _():
        halo_copy.wait_send()

    returned(3)
    result = result + share(3)
    finish_mix(0)
    for k in (1, 2):
        returned(k)
        result = result + share(k)
    exp_out[...] = result.astype(bf16)

    left(xs_m, 6)
    left(zs.at[pl.ds(1, 3)], 4)


def store_kernel(mix_ref, exp_ref, mix_hbm, exp_hbm, sem):
    stores = [
        pltpu.make_async_copy(mix_ref, mix_hbm, sem.at[0]),
        pltpu.make_async_copy(exp_ref, exp_hbm, sem.at[1]),
    ]
    for c in stores:
        c.start()
    for c in stores:
        c.wait()


def fused(
    mix_input,
    group_weight,
    pool_gain,
    branch_weight,
    exp_input,
    norm_gain,
    routes,
    route_weights,
    gate_weight,
    up_weight,
    down_weight,
):
    tokens, width = exp_input.shape
    rows_mix, channels = mix_input.shape
    hidden = gate_weight.shape[2]
    quarter = width // 4
    cap = 3 * tokens // 4
    hid_tiles = hidden // lanes
    half_mix = rows_mix // 2
    vmem = pl.BlockSpec(memory_space=pltpu.VMEM)
    anywhere = pl.BlockSpec(memory_space=pl.ANY)
    dma = pltpu.SemaphoreType.DMA
    mix_out, exp_out = pl.pallas_call(
        fused_kernel,
        out_shape=(
            pltpu.VMEM((rows_mix, quarter), bf16),
            pltpu.VMEM((tokens, quarter), bf16),
        ),
        in_specs=[anywhere] * 11,
        out_specs=(vmem, vmem),
        scratch_shapes=[
            pltpu.VMEM((tokens, width), bf16),
            pltpu.VMEM((1, width), f32),
            pltpu.VMEM((2, tokens), jnp.int32),
            pltpu.VMEM((2, tokens), f32),
            pltpu.VMEM((rows_mix, channels), bf16),
            pltpu.VMEM((1, 4 * channels), f32),
            pltpu.VMEM((hid_tiles, width, 2 * lanes), bf16),
            pltpu.VMEM((4, hidden, quarter), bf16),
            pltpu.VMEM((4, channels, quarter), bf16),
            pltpu.VMEM((channels // lanes, lanes, lanes), bf16),
            pltpu.VMEM((4, tokens, quarter), bf16),
            pltpu.VMEM((4, cap, quarter), bf16),
            pltpu.VMEM((4, 4, cap, quarter), bf16),
            pltpu.VMEM((4, hid_tiles, cap, 2 * lanes), f32),
            pltpu.VMEM((4, cap, hidden), bf16),
            pltpu.VMEM((16, channels), bf16),
            pltpu.VMEM((rows_mix, channels), bf16),
            pltpu.VMEM((2, 2, half_mix, quarter), f32),
            pltpu.VMEM((2, 2, half_mix, quarter), bf16),
            pltpu.VMEM((2, 2, half_mix, quarter), bf16),
            pltpu.VMEM((2, half_mix, quarter), bf16),
            pltpu.VMEM((2, half_mix, quarter), bf16),
            pltpu.VMEM((2, 4, cap, quarter), f32),
            pltpu.VMEM((2, 4, cap, quarter), bf16),
            pltpu.VMEM((2, 4, cap, quarter), bf16),
            pltpu.VMEM((4, cap, quarter), bf16),
            pltpu.VMEM((4, cap, quarter), bf16),
            pltpu.VMEM((4, cap, quarter), bf16),
            pltpu.VMEM((4, cap, quarter), bf16),
            dma((5,)),
            dma((6,)),
            dma((7,)),
            dma((4, pieces)),
            dma((2, pieces)),
            dma((2, 3)),
            dma((2, 4)),
            dma((4, pieces)),
            dma((3,)),
            dma((2, 3)),
            dma((2,)),
        ],
        compiler_params=pltpu.CompilerParams(
            collective_id=0, has_side_effects=True, vmem_limit_bytes=56 << 20
        ),
    )(
        exp_input,
        norm_gain.reshape(1, -1),
        routes.T,
        route_weights.T,
        mix_input,
        pool_gain.reshape(1, -1),
        group_weight,
        branch_weight,
        gate_weight,
        up_weight,
        down_weight,
    )
    return pl.pallas_call(
        store_kernel,
        out_shape=(
            jax.ShapeDtypeStruct((rows_mix, quarter), bf16),
            jax.ShapeDtypeStruct((tokens, quarter), bf16),
        ),
        in_specs=[vmem] * 2,
        out_specs=(anywhere, anywhere),
        scratch_shapes=[dma((2,))],
    )(
        pltpu.with_memory_space_constraint(mix_out, pltpu.VMEM),
        pltpu.with_memory_space_constraint(exp_out, pltpu.VMEM),
    )


def fits(mesh, args):
    mix, group, _, _, tok, _, routes, _, gate, _, _ = args
    ep, tp, grp = (mesh.shape[k] for k in ("ep", "tp", "grp"))
    if ep != 4 or tp != 4 or routes.shape[1] != 2 or gate.shape[0] != ep:
        return False
    rows, channels = mix.shape[0] // (grp * ep), mix.shape[1] // tp
    tokens, quarter = tok.shape[0] // (grp * ep), tok.shape[1] // tp
    return (
        group.shape[1] == lanes
        and channels % (4 * lanes) == 0
        and channels == quarter
        and rows % 32 == 0
        and tokens % 64 == 0
        and gate.shape[2] % (tp * lanes) == 0
        and gate.shape[1] * gate.shape[2] <= 1 << 23
        and rows <= 512
        and tokens <= 256
    )


def solution(mesh):
    def run(*args):
        body = fused if fits(mesh, args) else on_device
        return jax.shard_map(
            body,
            mesh=mesh,
            in_specs=(
                P(("grp", "ep"), "tp"),
                P(),
                P(),
                P("tp", None),
                P(("grp", "ep"), None),
                P(),
                P(("grp", "ep"), None),
                P(("grp", "ep"), None),
                P("ep", None, "tp"),
                P("ep", None, "tp"),
                P("ep", "tp", None),
            ),
            out_specs=(P(("grp", "ep"), "tp"), P(("grp", "ep"), "tp")),
            check_vma=False,
        )(*args)

    return run
```

```python
import functools

import jax
import jax.numpy as jnp
from jax import lax
from jax.experimental import pallas as pl
from jax.experimental.pallas import tpu as pltpu
from jax.sharding import PartitionSpec as P

windows = (2, 4, 8, 16)
epsilon = 1e-06


def shifted(block, axis, distance):
    devices = range(lax.axis_size(axis))
    route = [(i - distance, i) for i in devices if i - distance in devices]
    return lax.ppermute(block, axis, route)


def trailing_sums(extended, rows):
    span_two = extended[1:] + extended[:-1]
    span_four = span_two[2:] + span_two[:-2]
    span_eight = span_four[4:] + span_four[:-4]
    span_sixteen = span_eight[8:] + span_eight[:-8]
    return [span_two[-rows:], span_four[-rows:], span_eight[-rows:], span_sixteen]


def pooled_deviation(extended, positions, group_ids, group_width, rows):
    sums = trailing_sums(extended, rows)
    current = extended[-rows:]
    window_id = jnp.repeat(group_ids % 4, group_width)
    result = jnp.zeros_like(current)
    for window_level, window_len in enumerate(windows):
        counted = jnp.minimum(positions + 1, window_len).astype(jnp.float32)[:, None]
        result = jnp.where(
            window_id[None, :] == window_level, sums[window_level] / counted - current, result
        )
    return result


def on_device(
    mix_input,
    group_weight,
    pool_gain,
    branch_weight,
    exp_input,
    norm_gain,
    routes,
    route_weights,
    gate_weight,
    up_weight,
    down_weight,
):
    tp_rank = lax.axis_index("tp")
    ep_rank = lax.axis_index("ep")
    rows_mix, channels = mix_input.shape
    group_width = group_weight.shape[1]
    group_count = channels // group_width
    first_group = tp_rank * group_count
    last_rows = mix_input[rows_mix - 15 :]
    before = shifted(last_rows, "ep", 1)
    extended = jnp.concatenate([before, mix_input], axis=0).astype(jnp.float32)
    positions = ep_rank * rows_mix + jnp.arange(rows_mix, dtype=jnp.int32)
    group_ids = first_group + jnp.arange(group_count, dtype=jnp.int32)
    deviation = pooled_deviation(extended, positions, group_ids, group_width, rows_mix).astype(
        jnp.bfloat16
    )
    own_groups = lax.dynamic_slice_in_dim(group_weight, first_group, group_count, 0)
    grouped = jnp.einsum(
        "rgc,gcd->rgd",
        deviation.reshape(rows_mix, group_count, group_width),
        own_groups,
        preferred_element_type=jnp.float32,
    ).reshape(rows_mix, channels)
    own_gain = lax.dynamic_slice_in_dim(pool_gain, first_group * group_width, channels, 0)
    pooled = (grouped * own_gain).astype(jnp.bfloat16)
    tok_rows, width = exp_input.shape
    columns = width // lax.axis_size("tp")
    experts_all = lax.axis_size("ep")
    capacity = 3 * tok_rows // experts_all
    floated = exp_input.astype(jnp.float32)
    normed = (
        floated
        * lax.rsqrt(jnp.mean(floated * floated, axis=1, keepdims=True) + epsilon)
        * norm_gain
    ).astype(jnp.bfloat16)
    flat_expert = routes.reshape(-1)
    assignments = flat_expert.shape[0]
    onehot = (flat_expert[:, None] == jnp.arange(experts_all, dtype=jnp.int32)[None, :]).astype(
        jnp.int32
    )
    slot_rank = jnp.sum((jnp.cumsum(onehot, axis=0) - onehot) * onehot, axis=1)
    slot_index = flat_expert * capacity + slot_rank
    token_of = jnp.arange(assignments, dtype=jnp.int32) // routes.shape[1]
    slot_token = (
        jnp.full((experts_all * capacity,), tok_rows, jnp.int32).at[slot_index].set(token_of)
    )
    padded = jnp.concatenate([normed, jnp.zeros((1, width), jnp.bfloat16)], axis=0)
    w_gate = gate_weight[0]
    w_up = up_weight[0]
    w_down = down_weight[0]
    arrived_rows = experts_all * capacity
    own_columns = lax.dynamic_slice_in_dim(padded, tp_rank * columns, columns, 1)
    outgoing = own_columns[slot_token].reshape(experts_all, capacity, columns)
    arrived = lax.all_to_all(outgoing, "ep", split_axis=0, concat_axis=0, tiled=True).reshape(
        arrived_rows, columns
    )
    section = lax.all_gather(arrived, "tp", axis=1, tiled=True)
    gate_pre = jnp.dot(section, w_gate, preferred_element_type=jnp.float32)
    up_pre = jnp.dot(section, w_up, preferred_element_type=jnp.float32)
    hidden = (jax.nn.silu(gate_pre) * up_pre).astype(jnp.bfloat16)
    weight_cols = branch_weight
    mix_sum = lax.psum_scatter(
        lax.dot_general(
            weight_cols, pooled, (((0,), (1,)), ((), ())), preferred_element_type=jnp.float32
        ).astype(jnp.bfloat16),
        "tp",
        scatter_dimension=0,
        tiled=True,
    )
    weight_cols = w_down
    exp_sum = lax.psum_scatter(
        lax.dot_general(
            weight_cols, hidden, (((0,), (1,)), ((), ())), preferred_element_type=jnp.float32
        ).astype(jnp.bfloat16),
        "tp",
        scatter_dimension=0,
        tiled=True,
    )
    mix_out = mix_sum.T
    results = exp_sum.reshape(columns, experts_all, capacity)
    returned = lax.all_to_all(results, "ep", split_axis=1, concat_axis=1, tiled=True).reshape(
        columns, experts_all * capacity
    )
    picked = returned[:, slot_index].astype(jnp.float32)
    weighted = picked * route_weights.reshape(-1)[None, :]
    combined = jnp.sum(weighted.reshape(columns, tok_rows, routes.shape[1]), axis=2)
    exp_out = combined.T.astype(jnp.bfloat16)
    return (mix_out, exp_out)


lanes = 128
pieces = 2
MESH = pl.DeviceIdType.MESH
f32 = jnp.float32
bf16 = jnp.bfloat16


def fused_kernel(
    x_hbm,
    norm_hbm,
    routes_hbm,
    weights_hbm,
    mix_hbm,
    gain_hbm,
    groups_hbm,
    branch_hbm,
    gate_hbm,
    up_hbm,
    down_hbm,
    mix_out,
    exp_out,
    x_ref,
    norm_ref,
    routes_ref,
    weights_ref,
    mix_ref,
    gain_ref,
    wgu,
    wd,
    wb,
    gw,
    xn,
    sb,
    xg,
    gu,
    hid,
    halo,
    pooled,
    keep_m,
    ps_m,
    pr_m,
    xs_m,
    xr_m,
    keep,
    ps,
    pr,
    xs,
    xr,
    zs,
    zr,
    w_sem,
    i_sem,
    s_sem,
    d_recv,
    f_recv,
    g_recv,
    p_recv,
    r_recv,
    z_recv,
    m_recv,
    h_sem,
):
    z = lax.axis_index("ep")
    t = lax.axis_index("tp")
    near = t + 1 - 2 * (t % 2)
    across = (t + 2) % 4
    diagonal = (near + 2) % 4
    inner = ((z + 1) // 2) % 2
    peers = [z, z + 1 - 2 * (z % 2), 3 - z, (z + 2) % 4]
    landing = 3 - inner
    slots = [0, 3, 2 - inner, 1 + inner]
    homes = [0, 2 + inner, 3 - 2 * inner, 1 + inner]
    home_of = [
        z,
        inner * peers[3] + (1 - inner) * peers[2],
        inner * peers[1] + (1 - inner) * peers[3],
        inner * peers[2] + (1 - inner) * peers[1],
    ]
    second = inner * across + (1 - inner) * near
    third = inner * near + (1 - inner) * across
    early = [None, (t, near), (t, second), (t, third)]
    late = [None, (across, diagonal), (third, diagonal), (second, diagonal)]
    tokens, width = x_ref.shape
    quarter = width // 4
    cap = xg.shape[2]
    piece = cap // pieces
    hid_tiles = gate_hbm.shape[2] // lanes
    rows_mix, channels = mix_ref.shape
    half_mix = rows_mix // 2
    group_count = channels // lanes

    barrier = pltpu.get_barrier_semaphore()
    for k in (1, 2, 3):
        pl.semaphore_signal(barrier, inc=1, device_id={"ep": peers[k]}, device_id_type=MESH)
    for k in (near, across):
        pl.semaphore_signal(barrier, inc=1, device_id={"tp": k}, device_id_type=MESH)

    pairs = (
        (routes_hbm, routes_ref),
        (weights_hbm, weights_ref),
        (x_hbm, x_ref),
        (norm_hbm, norm_ref),
        (mix_hbm, mix_ref),
        (gain_hbm, gain_ref),
    )
    part = tokens // 4
    load_x = [
        pltpu.make_async_copy(x_hbm.at[pl.ds(i * part, part)], x_ref.at[pl.ds(i * part, part)], i_sem.at[2])
        for i in range(4)
    ]
    load_i = [pltpu.make_async_copy(src, dst, i_sem.at[i]) for i, (src, dst) in enumerate(pairs)]
    front = (hid_tiles + 1) // 2
    loads = []
    for i in range(2 * hid_tiles):
        src = gate_hbm if i < hid_tiles else up_hbm
        at = (i % hid_tiles) * lanes
        loads.append(
            pltpu.make_async_copy(
                src.at[0, :, pl.ds(at, lanes)],
                wgu.at[i // 2, :, pl.ds((i % 2) * lanes, lanes)],
                w_sem.at[0 if i // 2 < front else 1],
            )
        )
    load_b = [
        pltpu.make_async_copy(branch_hbm.at[:, pl.ds(k * quarter, quarter)], wb.at[k], w_sem.at[2])
        for k in range(4)
    ]
    load_d = [
        pltpu.make_async_copy(down_hbm.at[0, :, pl.ds(k * quarter, quarter)], wd.at[k], w_sem.at[3])
        for k in range(4)
    ]
    load_g = pltpu.make_async_copy(groups_hbm.at[pl.ds(t * group_count, group_count)], gw, w_sem.at[4])

    def loaded(ref, i):
        pltpu.make_async_copy(ref, ref, w_sem.at[i]).wait()

    for c in load_i[:2] + load_x + load_i[3:]:
        c.start()

    def remote(src, dst, send, recv, who):
        return pltpu.make_async_remote_copy(
            src_ref=src, dst_ref=dst, send_sem=send, recv_sem=recv, device_id=who, device_id_type=MESH
        )

    for c in load_i[:2]:
        c.wait()
    lane = lax.broadcasted_iota(jnp.int32, (tokens, lanes), 1)
    square = (tokens, tokens)
    diagonal_mask = lax.broadcasted_iota(jnp.int32, square, 0) == lax.broadcasted_iota(jnp.int32, square, 1)

    def column(row):
        spread = jnp.broadcast_to(row, square)
        return jnp.sum(jnp.where(diagonal_mask, spread, jnp.zeros_like(spread)), axis=1, keepdims=True)

    r0 = column(routes_ref[0:1, :].astype(f32)).astype(jnp.int32)
    r1 = column(routes_ref[1:2, :].astype(f32)).astype(jnp.int32)
    w0 = column(weights_ref[0:1, :])
    w1 = column(weights_ref[1:2, :])
    member = ((r0 == lane) | (r1 == lane)).astype(f32)
    above = (
        lax.broadcasted_iota(jnp.int32, (tokens, tokens), 0)
        > lax.broadcasted_iota(jnp.int32, (tokens, tokens), 1)
    ).astype(f32)
    rank = jnp.dot(above.astype(bf16), member.astype(bf16), preferred_element_type=f32)
    slot_lane = lax.broadcasted_iota(jnp.int32, (tokens, cap), 1)
    places = []
    shares = []
    for k in range(4):
        own = jnp.sum(jnp.where(lane == peers[k], rank, 0.0), axis=1, keepdims=True).astype(jnp.int32)
        named = (r0 == peers[k]) | (r1 == peers[k])
        slot = jnp.where(named, own, cap)
        places.append((slot_lane == slot).astype(f32).astype(bf16))
        shares.append(
            jnp.where(r0 == peers[k], w0, 0.0)
            + jnp.where(r1 == peers[k], w1, 0.0)
        )

    for c in load_i[2:4]:
        c.wait()
    for c in [load_g] + load_b + loads + load_d:
        c.start()
    floated = x_ref[...].astype(f32)
    scale = lax.rsqrt(jnp.mean(floated * floated, axis=1, keepdims=True) + epsilon)
    own_at = pl.ds(pl.multiple_of(t * quarter, quarter), quarter)
    own_cols = (x_ref[:, own_at].astype(f32) * scale * norm_ref[:, own_at]).astype(bf16)

    def gathered(k, block):
        return lax.dot_general(
            places[k], block, (((0,), (0,)), ((), ())), preferred_element_type=f32
        ).astype(bf16)

    def if_inner(step, *k):
        pl.when(inner == 1)(lambda: step(*k))

    def if_outer(step, *k):
        pl.when(inner == 0)(lambda: step(*k))

    for k in (2, 3):
        sb[k] = gathered(k, own_cols)
    for c in load_i[4:]:
        c.wait()
    pl.semaphore_wait(barrier, 5)

    def d_z(j, p):
        rows = pl.ds(p * piece, piece)
        q = across if j == 1 else t
        slot = 1 if j < 2 else landing
        at = j if j < 2 else landing
        return remote(
            sb.at[j, rows],
            xg.at[q, slot, rows],
            s_sem.at[0],
            d_recv.at[at, p],
            {"ep": peers[max(j, 1)]},
        )

    halo_copy = remote(
        mix_ref.at[pl.ds(rows_mix - 16, 16), :], halo, h_sem.at[0], h_sem.at[1], {"ep": (z + 1) % 4}
    )

    @pl.when(z < 3)
    def _():
        halo_copy.start()

    def send_rows(order):
        for j in order:
            for p in range(pieces):
                d_z(j, p).start()

    if_outer(send_rows, (2, 3))
    if_inner(send_rows, (3, 2))
    xn_val = (floated * scale * norm_ref[...]).astype(bf16)
    for k in range(4):
        xn[k] = xn_val[:, k * quarter : (k + 1) * quarter]
    sb[0] = gathered(1, own_cols)
    sb[1] = gathered(1, xn[across])
    send_rows((0, 1))
    for q in range(4):
        xg[q, 0] = gathered(0, xn[q])

    def arrival(at, q, slot, p):
        rows = pl.ds(p * piece, piece)
        return remote(
            sb.at[0, rows], xg.at[q, slot, rows], s_sem.at[0], d_recv.at[at, p], {"ep": peers[1]}
        )

    def forward(i, q, slot, p):
        rows = pl.ds(p * piece, piece)
        block = xg.at[q, slot, rows]
        landed = f_recv.at[slot - 2, p] if i == 0 else g_recv.at[i - 1, slot - 1]
        return remote(block, block, s_sem.at[1], landed, {"tp": across if i == 0 else near})

    def from_z(k):
        if k == 1:
            for p in range(pieces):
                arrival(0, t, 1, p).wait_recv()
                forward(1, t, 1, p).start()
            for p in range(pieces):
                arrival(1, across, 1, p).wait_recv()
                forward(2, across, 1, p).start()
            return
        for p in range(pieces):
            arrival(k, t, k, p).wait_recv()
            forward(0, t, k, p).start()
            forward(1, t, k, p).start()

    def from_x(k):
        for p in range(pieces):
            forward(0, across, k, p).wait_recv()
            forward(2, across, k, p).start()

    def near_own(k):
        block = xg.at[near, k]
        remote(block, block, s_sem.at[1], g_recv.at[0, k - 1], {"tp": near}).wait_recv()

    def near_other(k):
        block = xg.at[diagonal, k]
        remote(block, block, s_sem.at[1], g_recv.at[1, k - 1], {"tp": near}).wait_recv()

    def mix_half(h):
        rows = slice(h * half_mix, (h + 1) * half_mix)
        position = z * rows_mix + h * half_mix + lax.broadcasted_iota(jnp.int32, (half_mix, lanes), 0)
        for g in range(group_count):
            cols = slice(g * lanes, (g + 1) * lanes)
            current = mix_ref[rows, cols].astype(f32)
            if h == 0:
                past = halo[:, cols].astype(f32)
            else:
                past = mix_ref[h * half_mix - 16 : h * half_mix, cols].astype(f32)
            total = jnp.concatenate([past, current], axis=0)
            level = g % 4
            for step in range(level + 1):
                total = total + pltpu.roll(total, 1 << step, 0)
            counted = jnp.minimum(position + 1, windows[level]).astype(f32)
            deviation = (total[16:] / counted - current).astype(bf16)
            grouped = jnp.dot(deviation, gw[g], preferred_element_type=f32)
            gain = gain_ref[:, pl.ds(pl.multiple_of(t * channels + g * lanes, lanes), lanes)]
            pooled[rows, cols] = (grouped * gain).astype(bf16)
        for i, q in enumerate((diagonal, near)):
            ps_m[h, i] = jnp.dot(pooled[rows], wb[q], preferred_element_type=f32).astype(bf16)
        for i, q in enumerate((across, t)):
            keep_m[h, i] = jnp.dot(pooled[rows], wb[q], preferred_element_type=f32)
        for i in range(2):
            m_p(h, i).start()

    def m_p(h, i):
        return remote(ps_m.at[h, i], pr_m.at[h, i], s_sem.at[5], m_recv.at[h, i], {"tp": near})

    def m_x(h):
        return remote(xs_m.at[h], xr_m.at[h], s_sem.at[6], m_recv.at[h, 2], {"tp": across})

    def send_mix(h):
        m_p(h, 0).wait_recv()
        xs_m[h] = (keep_m[h, 0] + pr_m[h, 0].astype(f32)).astype(bf16)
        m_x(h).start()

    def finish_mix(h):
        m_p(h, 1).wait_recv()
        m_x(h).wait_recv()
        total = keep_m[h, 1] + pr_m[h, 1].astype(f32) + xr_m[h].astype(f32)
        mix_out[h * half_mix : (h + 1) * half_mix] = total.astype(bf16)

    def expand(k, blocks, first, last):
        for n in range(first, last):
            if k == 0 and n == 0:
                loaded(wgu.at[pl.ds(0, front)], 0)
            if k == 0 and n == front:
                loaded(wgu.at[pl.ds(front, hid_tiles - front)], 1)
            total = None if blocks is None or blocks is early[k] else gu[k, n]
            for q in range(4) if blocks is None else blocks:
                rows = pl.ds(q * quarter if blocks is None else pl.multiple_of(q * quarter, quarter), quarter)
                part = jnp.dot(xg[q, slots[k]], wgu[n, rows, :], preferred_element_type=f32)
                total = part if total is None else total + part
            gu[k, n] = total

    def expand_early(k, first, last):
        expand(k, early[k], first, last)

    def activate(k):
        for i in range(hid_tiles):
            m = hid_tiles + i
            gate = gu[k, i // 2, :, (i % 2) * lanes : (i % 2 + 1) * lanes]
            up = gu[k, m // 2, :, (m % 2) * lanes : (m % 2 + 1) * lanes]
            hid[k, :, i * lanes : (i + 1) * lanes] = (gate / (1.0 + jnp.exp(-gate)) * up).astype(bf16)

    def r_p(i, k):
        return remote(ps.at[i, k], pr.at[i, k], s_sem.at[2], p_recv.at[i, k], {"tp": near})

    def r_x(k, p):
        rows = pl.ds(p * piece, piece)
        return remote(xs.at[k, rows], xr.at[k, rows], s_sem.at[3], r_recv.at[k, p], {"tp": across})

    def r_z(k, p):
        rows = pl.ds(p * piece, piece)
        return remote(
            zs.at[k, rows],
            zr.at[homes[k], rows],
            s_sem.at[4],
            z_recv.at[homes[k] - 1],
            {"ep": home_of[k]},
        )

    def project(k, first=0, last=4):
        for i, q in list(enumerate((diagonal, near, across, t)))[first:last]:
            part = jnp.dot(hid[k], wd[q], preferred_element_type=f32)
            if i < 2:
                ps[i, k] = part.astype(bf16)
            else:
                keep[i - 2, k] = part
            if i == 0:
                r_p(0, k).start()
        if last == 4:
            r_p(1, k).start()

    def send_x(k):
        r_p(0, k).wait_recv()
        for p in range(pieces):
            rows = slice(p * piece, (p + 1) * piece)
            xs[k, rows] = (keep[0, k, rows] + pr[0, k, rows].astype(f32)).astype(bf16)
            r_x(k, p).start()

    def send_z(k, first=0, last=pieces):
        if first == 0:
            r_p(1, k).wait_recv()
        for p in range(first, last):
            rows = slice(p * piece, (p + 1) * piece)
            r_x(k, p).wait_recv()
            zs[k, rows] = (keep[1, k, rows] + pr[1, k, rows].astype(f32) + xr[k, rows].astype(f32)).astype(bf16)
            if k > 0:
                r_z(k, p).start()

    def share(k):
        block = zs[0] if k == 0 else zr[k]
        return shares[k] * jnp.dot(places[k], block, preferred_element_type=f32)

    def returned(k):
        remote(zs.at[k], zr.at[k], s_sem.at[4], z_recv.at[k - 1], {"ep": peers[k]}).wait_recv()

    def left(ref, i):
        remote(ref, ref, s_sem.at[i], s_sem.at[i], {"tp": near}).wait_send()

    half = hid_tiles // 2
    load_g.wait()
    loaded(wb, 2)
    mix_half(1)
    expand(0, None, 0, half)
    send_mix(1)
    expand(0, None, half, hid_tiles)
    activate(0)
    loaded(wd, 3)
    project(0)
    if_outer(from_z, 3)

    @pl.when(z == 0)
    def _():
        halo[...] = jnp.zeros_like(halo)

    @pl.when(z > 0)
    def _():
        halo_copy.wait_recv()

    mix_half(0)
    if_inner(from_z, 3)
    near_own(3)
    expand(1, early[1], 0, hid_tiles)
    if_outer(from_z, 2)
    if_outer(from_x, 3)
    if_inner(from_x, 3)
    from_z(1)
    if_inner(from_z, 2)
    expand(1, late[1][:1], 0, hid_tiles)
    if_outer(near_own, 2)
    if_outer(send_mix, 0)
    expand(2, early[2], 0, hid_tiles)
    if_inner(send_x, 0)
    near_other(3)
    expand(1, late[1][1:], 0, hid_tiles)
    activate(1)
    project(1)
    if_outer(from_x, 2)
    if_outer(send_x, 1)
    if_outer(send_x, 0)
    if_outer(expand_early, 3, 0, hid_tiles)
    if_inner(near_own, 1)
    if_inner(near_other, 1)
    if_outer(near_other, 2)
    expand(2, late[2], 0, half)
    if_inner(send_x, 1)
    expand(2, late[2], half, hid_tiles)
    activate(2)
    project(2, 0, 2)
    if_inner(from_x, 2)
    project(2, 2, 4)
    if_inner(near_own, 2)
    if_inner(expand_early, 3, 0, half)
    if_inner(send_x, 2)
    if_inner(expand_early, 3, half, hid_tiles)
    if_outer(near_own, 1)
    if_outer(near_other, 1)
    if_inner(near_other, 2)
    expand(3, late[3], 0, half)
    if_outer(send_x, 2)
    expand(3, late[3], half, hid_tiles)
    activate(3)
    if_outer(send_z, 1)
    if_inner(send_z, 1, 0, 1)
    project(3)
    if_inner(send_z, 1, 1, pieces)
    send_x(3)
    if_outer(send_z, 2, 0, 1)
    if_outer(send_z, 3, 0, 1)
    if_outer(send_z, 2, 1, pieces)
    if_outer(send_z, 3, 1, pieces)
    if_inner(send_z, 2)
    if_inner(send_mix, 0)
    if_inner(send_z, 3)
    send_z(0)
    finish_mix(1)
    result = share(0)
    left(sb, 0)
    left(xg.at[pl.ds(0, 2)], 1)
    left(ps, 2)
    left(xs, 3)
    left(ps_m, 5)

    @pl.when(z < 3)
    def _():
        halo_copy.wait_send()

    returned(3)
    result = result + share(3)
    finish_mix(0)
    for k in (1, 2):
        returned(k)
        result = result + share(k)
    exp_out[...] = result.astype(bf16)

    left(xs_m, 6)
    left(zs.at[pl.ds(1, 3)], 4)


def store_kernel(mix_ref, exp_ref, mix_hbm, exp_hbm, sem):
    stores = [
        pltpu.make_async_copy(mix_ref, mix_hbm, sem.at[0]),
        pltpu.make_async_copy(exp_ref, exp_hbm, sem.at[1]),
    ]
    for c in stores:
        c.start()
    for c in stores:
        c.wait()


def fused(
    mix_input,
    group_weight,
    pool_gain,
    branch_weight,
    exp_input,
    norm_gain,
    routes,
    route_weights,
    gate_weight,
    up_weight,
    down_weight,
):
    tokens, width = exp_input.shape
    rows_mix, channels = mix_input.shape
    hidden = gate_weight.shape[2]
    quarter = width // 4
    cap = 3 * tokens // 4
    hid_tiles = hidden // lanes
    half_mix = rows_mix // 2
    vmem = pl.BlockSpec(memory_space=pltpu.VMEM)
    anywhere = pl.BlockSpec(memory_space=pl.ANY)
    dma = pltpu.SemaphoreType.DMA
    mix_out, exp_out = pl.pallas_call(
        fused_kernel,
        out_shape=(
            pltpu.VMEM((rows_mix, quarter), bf16),
            pltpu.VMEM((tokens, quarter), bf16),
        ),
        in_specs=[anywhere] * 11,
        out_specs=(vmem, vmem),
        scratch_shapes=[
            pltpu.VMEM((tokens, width), bf16),
            pltpu.VMEM((1, width), f32),
            pltpu.VMEM((2, tokens), jnp.int32),
            pltpu.VMEM((2, tokens), f32),
            pltpu.VMEM((rows_mix, channels), bf16),
            pltpu.VMEM((1, 4 * channels), f32),
            pltpu.VMEM((hid_tiles, width, 2 * lanes), bf16),
            pltpu.VMEM((4, hidden, quarter), bf16),
            pltpu.VMEM((4, channels, quarter), bf16),
            pltpu.VMEM((channels // lanes, lanes, lanes), bf16),
            pltpu.VMEM((4, tokens, quarter), bf16),
            pltpu.VMEM((4, cap, quarter), bf16),
            pltpu.VMEM((4, 4, cap, quarter), bf16),
            pltpu.VMEM((4, hid_tiles, cap, 2 * lanes), f32),
            pltpu.VMEM((4, cap, hidden), bf16),
            pltpu.VMEM((16, channels), bf16),
            pltpu.VMEM((rows_mix, channels), bf16),
            pltpu.VMEM((2, 2, half_mix, quarter), f32),
            pltpu.VMEM((2, 2, half_mix, quarter), bf16),
            pltpu.VMEM((2, 2, half_mix, quarter), bf16),
            pltpu.VMEM((2, half_mix, quarter), bf16),
            pltpu.VMEM((2, half_mix, quarter), bf16),
            pltpu.VMEM((2, 4, cap, quarter), f32),
            pltpu.VMEM((2, 4, cap, quarter), bf16),
            pltpu.VMEM((2, 4, cap, quarter), bf16),
            pltpu.VMEM((4, cap, quarter), bf16),
            pltpu.VMEM((4, cap, quarter), bf16),
            pltpu.VMEM((4, cap, quarter), bf16),
            pltpu.VMEM((4, cap, quarter), bf16),
            dma((5,)),
            dma((6,)),
            dma((7,)),
            dma((4, pieces)),
            dma((2, pieces)),
            dma((2, 3)),
            dma((2, 4)),
            dma((4, pieces)),
            dma((3,)),
            dma((2, 3)),
            dma((2,)),
        ],
        compiler_params=pltpu.CompilerParams(
            collective_id=0, has_side_effects=True, vmem_limit_bytes=56 << 20
        ),
    )(
        exp_input,
        norm_gain.reshape(1, -1),
        routes.T,
        route_weights.T,
        mix_input,
        pool_gain.reshape(1, -1),
        group_weight,
        branch_weight,
        gate_weight,
        up_weight,
        down_weight,
    )
    return pl.pallas_call(
        store_kernel,
        out_shape=(
            jax.ShapeDtypeStruct((rows_mix, quarter), bf16),
            jax.ShapeDtypeStruct((tokens, quarter), bf16),
        ),
        in_specs=[vmem] * 2,
        out_specs=(anywhere, anywhere),
        scratch_shapes=[dma((2,))],
    )(
        pltpu.with_memory_space_constraint(mix_out, pltpu.VMEM),
        pltpu.with_memory_space_constraint(exp_out, pltpu.VMEM),
    )


def fits(mesh, args):
    mix, group, _, _, tok, _, routes, _, gate, _, _ = args
    ep, tp, grp = (mesh.shape[k] for k in ("ep", "tp", "grp"))
    if ep != 4 or tp != 4 or routes.shape[1] != 2 or gate.shape[0] != ep:
        return False
    rows, channels = mix.shape[0] // (grp * ep), mix.shape[1] // tp
    tokens, quarter = tok.shape[0] // (grp * ep), tok.shape[1] // tp
    return (
        group.shape[1] == lanes
        and channels % (4 * lanes) == 0
        and channels == quarter
        and rows % 32 == 0
        and tokens % 64 == 0
        and gate.shape[2] % (tp * lanes) == 0
        and gate.shape[1] * gate.shape[2] <= 1 << 23
        and rows <= 512
        and tokens <= 256
    )


def solution(mesh):
    def run(*args):
        body = fused if fits(mesh, args) else on_device
        return jax.shard_map(
            body,
            mesh=mesh,
            in_specs=(
                P(("grp", "ep"), "tp"),
                P(),
                P(),
                P("tp", None),
                P(("grp", "ep"), None),
                P(),
                P(("grp", "ep"), None),
                P(("grp", "ep"), None),
                P("ep", None, "tp"),
                P("ep", None, "tp"),
                P("ep", "tp", None),
            ),
            out_specs=(P(("grp", "ep"), "tp"), P(("grp", "ep"), "tp")),
            check_vma=False,
        )(*args)

    return run
```
